128 devices in a mesh: sp: 16 (over z, y), tp: 8 (over x, core).
Axes of the slice: x: 4, y: 4, z: 4, core: 2. Of those that a mesh axis runs over, the one named last changes fastest.
Arguments:
- tokens: bfloat16 [16384, 2048], P('sp', 'tp'), may hold values from -16 to 16
- mix_gain: float32 [2048], replicated, may hold values from 0.1 to 1.9
- query_weight: bfloat16 [2048, 1024], P(None, 'tp'), may hold values from -0.125 to 0.125
- key_weight: bfloat16 [2048, 1024], P(None, 'tp'), may hold values from -0.125 to 0.125
- value_weight: bfloat16 [2048, 1024], P(None, 'tp'), may hold values from -0.125 to 0.125
- outer_gate_weight: bfloat16 [2048, 1024], P(None, 'tp'), may hold values from -0.125 to 0.125
- inner_gate_weight: bfloat16 [2048, 1024], P(None, 'tp'), may hold values from -0.125 to 0.125
- conv_input_weight: bfloat16 [2048, 1024], P(None, 'tp'), may hold values from -0.125 to 0.125
- query_gain: float32 [64], replicated, may hold values from 0.6 to 10
- key_gain: float32 [64], replicated, may hold values from 0.6 to 10
- gate_totals: float32 [16384, 16], P('sp', 'tp'), may hold values from -4096 to 0, as said below
- conv_taps: float32 [3, 1024], P(None, 'tp'), may hold values from -3 to 3
- attn_out_gain: float32 [1024], P('tp'), may hold values from 0.1 to 1.9
- conv_out_gain: float32 [1024], P('tp'), may hold values from 0.1 to 1.9
- attn_out_weight: bfloat16 [1024, 2048], P('tp'), may hold values from -0.125 to 0.125
- conv_out_weight: bfloat16 [1024, 2048], P('tp'), may hold values from -0.125 to 0.125
Outputs:
- mixed: bfloat16 [16384, 2048], P(('sp', 'tp'))
The draws below stay inside these ranges and needn't reach their ends.
Inputs may be any that keep to these rules, and one draw needn't show every extreme that they name: `gate_totals`: in every head the values never rise from one position to the next.
All inputs are finite; a program needn't handle non-finite values.
Results may differ from the reference program's by a relative error of at most 0.015.
The reference program's roundings to bfloat16 on the way count: a program that leaves them out, or rounds other values in their place, can miss the bound.
Values may be sent and summed in bfloat16 or wider, within the bound.
A program may use at most 64 MiB of HBM per device.

```python
import math
import jax
import jax.numpy as jnp
from jax import lax

D = 2048
HEAD_DIM = 64
ATTENTION_HEADS = 16
CONV_K = 3
TOK_DEV = 1024
ATTN_WIDTH = 1024
CONV_WIDTH = 1024
SEQUENCE_TOKENS = 16384
N_TP = 8


def draw_tokens(key, part):
    random_subkeys = jax.random.split(jax.random.fold_in(key, 101), 2)
    column = jnp.arange(D, dtype=jnp.float32) / D
    column_scale = 0.5 * jnp.exp(math.log(4.0) * column) * jax.random.uniform(random_subkeys[1], (D,), jnp.float32, 0.7, 1.4)
    normal_part = jax.random.normal(random_subkeys[0], (SEQUENCE_TOKENS, D), jnp.float32)
    return jnp.clip(normal_part * column_scale, -16.0, 16.0).astype(jnp.bfloat16)


def focus_gain(key):
    gain = jax.random.uniform(key, (HEAD_DIM,), jnp.float32, 0.6, 1.4)
    return gain


def draw_query_gain(key, part):
    return focus_gain(jax.random.fold_in(key, 211))


def draw_key_gain(key, part):
    return focus_gain(jax.random.fold_in(key, 307))


def draw_gate_totals(key, part):
    random_subkeys = jax.random.split(jax.random.fold_in(key, 401), 7)
    order = jax.random.permutation(random_subkeys[0], ATTENTION_HEADS)
    fast_path = order < ATTENTION_HEADS // 2
    slow_total = jax.random.uniform(random_subkeys[1], (ATTENTION_HEADS,), jnp.float32, 0.15, 0.5)
    quick_reach = jnp.exp(jax.random.uniform(random_subkeys[2], (ATTENTION_HEADS,), jnp.float32, math.log(30.0), math.log(100.0)))
    base_rate = jnp.where(fast_path, 1.0 / quick_reach, slow_total / SEQUENCE_TOKENS)
    block_factor = jnp.exp(jax.random.uniform(random_subkeys[3], (SEQUENCE_TOKENS // TOK_DEV, 1), jnp.float32, math.log(0.5), math.log(2.0)))
    block_rate = jnp.repeat(block_factor, TOK_DEV, axis=0)
    jitter = jnp.exp(jax.random.uniform(random_subkeys[4], (SEQUENCE_TOKENS, ATTENTION_HEADS), jnp.float32, math.log(0.5), math.log(2.0)))
    per_step_loss = base_rate[None, :] * block_rate * jitter
    spike_position = jax.random.randint(random_subkeys[5], (2,), 0, SEQUENCE_TOKENS)
    spike_hit = jnp.any(jnp.arange(SEQUENCE_TOKENS)[:, None] == spike_position[None, :], axis=1)
    spike_loss = jax.random.uniform(random_subkeys[6], (SEQUENCE_TOKENS, ATTENTION_HEADS), jnp.float32, 0.22, 0.51)
    per_step_loss = per_step_loss + jnp.where(spike_hit[:, None] & jnp.logical_not(fast_path)[None, :], spike_loss, 0.0)
    return -jnp.cumsum(per_step_loss, axis=0)


def block_levels(stream_key, shape, cuts, low, top_value):
    level, own = 1.0, jax.random.fold_in(stream_key, 6)
    for position, shards_of in cuts:
        draws = jnp.exp(jax.random.uniform(jax.random.fold_in(own, position), (shards_of,), jnp.float32, low / len(cuts), top_value / len(cuts)))
        level = level * jnp.repeat(draws, shape[position] // shards_of).reshape([-1 if axis == position else 1 for axis in range(len(shape))])
    return level


def centred(stream_key, shape, deviation, most, cuts=(), kind=jnp.bfloat16):
    array = deviation * jax.random.normal(stream_key, shape, jnp.float32)
    if cuts:
        array = array * block_levels(stream_key, shape, cuts, -0.22, 0.18)
    return jnp.clip(array, -most, most).astype(kind)


def setup_inputs(seed: int = 0) -> dict:
    key_of = jax.random.split(jax.random.key(seed), 17)
    return {
        "tokens": draw_tokens(jax.random.fold_in(key_of[16], 71), 0),
        "mix_gain": jnp.clip(1.0 + 0.18 * jax.random.normal(key_of[1], (D,), jnp.float32), 0.1, 1.9),
        "query_weight": centred(key_of[2], (D, ATTN_WIDTH), D ** -0.5, 0.125, ((1, 8),)),
        "key_weight": centred(key_of[3], (D, ATTN_WIDTH), D ** -0.5, 0.125, ((1, 8),)),
        "value_weight": centred(key_of[4], (D, ATTN_WIDTH), D ** -0.5, 0.125, ((1, 8),)),
        "outer_gate_weight": centred(key_of[5], (D, CONV_WIDTH), D ** -0.5, 0.125, ((1, 8),)),
        "inner_gate_weight": centred(key_of[6], (D, CONV_WIDTH), D ** -0.5, 0.125, ((1, 8),)),
        "conv_input_weight": centred(key_of[7], (D, CONV_WIDTH), D ** -0.5, 0.125, ((1, 8),)),
        "query_gain": draw_query_gain(jax.random.fold_in(key_of[16], 71), 0),
        "key_gain": draw_key_gain(jax.random.fold_in(key_of[16], 71), 0),
        "gate_totals": draw_gate_totals(jax.random.fold_in(key_of[16], 71), 0),
        "conv_taps": centred(key_of[11], (CONV_K, CONV_WIDTH), 0.6, 3.0, ((1, 8),), jnp.float32),
        "attn_out_gain": jnp.clip(1.0 + 0.18 * jax.random.normal(key_of[12], (ATTN_WIDTH,), jnp.float32), 0.1, 1.9),
        "conv_out_gain": jnp.clip(1.0 + 0.18 * jax.random.normal(key_of[13], (CONV_WIDTH,), jnp.float32), 0.1, 1.9),
        "attn_out_weight": centred(key_of[14], (ATTN_WIDTH, D), (ATTN_WIDTH + CONV_WIDTH) ** -0.5, 0.125, ((0, 8),)),
        "conv_out_weight": centred(key_of[15], (CONV_WIDTH, D), (ATTN_WIDTH + CONV_WIDTH) ** -0.5, 0.125, ((0, 8),)),
    }


NORM_EPSILON = 1e-06

def head_norm(values, head_dim, gain):
    row_count = values.shape[0]
    grouped = values.reshape(row_count, -1, head_dim)
    normed = grouped * lax.rsqrt(lax.optimization_barrier(jnp.mean(grouped * grouped, axis=2, keepdims=True)) + NORM_EPSILON)
    return (normed * gain.reshape(-1, head_dim)).reshape(row_count, -1)

def settle(values):
    return lax.optimization_barrier(values.astype(jnp.bfloat16)).astype(jnp.float32)

def reference(tokens, mix_gain, query_weight, key_weight, value_weight, outer_gate_weight, inner_gate_weight, conv_input_weight, query_gain, key_gain, gate_totals, conv_taps, attn_out_gain, conv_out_gain, attn_out_weight, conv_out_weight):
    widened = tokens.astype(jnp.float32)
    row_scale = lax.rsqrt(lax.optimization_barrier(jnp.sum(widened * widened, axis=1, keepdims=True)) / D + NORM_EPSILON)
    scaled = (widened * mix_gain).astype(jnp.bfloat16)

    def project(weight):
        return row_scale * jnp.dot(scaled, weight, preferred_element_type=jnp.float32)
    queries = settle(head_norm(project(query_weight), HEAD_DIM, query_gain))
    key_rows = settle(head_norm(project(key_weight), HEAD_DIM, key_gain))
    value_rows = settle(project(value_weight))
    query_span = math.gcd(SEQUENCE_TOKENS, 512)
    score_scale = HEAD_DIM ** (-0.5)
    positions = jnp.arange(SEQUENCE_TOKENS, dtype=jnp.int32)

    def one_head(head_index):
        offset = (head_index * HEAD_DIM).astype(jnp.int32)
        head_queries = lax.dynamic_slice_in_dim(queries, offset, HEAD_DIM, 1)
        head_keys = lax.dynamic_slice_in_dim(key_rows, offset, HEAD_DIM, 1)
        head_values = lax.dynamic_slice_in_dim(value_rows, offset, HEAD_DIM, 1)
        head_gates = lax.dynamic_slice_in_dim(gate_totals, head_index.astype(jnp.int32), 1, 1)[:, 0]

        def one_block(block_index):
            start = (block_index * query_span).astype(jnp.int32)
            block_queries = lax.dynamic_slice_in_dim(head_queries, start, query_span, 0)
            block_gates = lax.dynamic_slice_in_dim(head_gates, start, query_span, 0)
            scores = jnp.dot(block_queries, head_keys.T, precision=lax.Precision.HIGHEST) * score_scale
            scores = scores + block_gates[:, None] - head_gates[None, :]
            allowed = positions[None, :] <= (start + jnp.arange(query_span, dtype=jnp.int32))[:, None]
            row_max = lax.optimization_barrier(jnp.max(jnp.where(allowed, scores, -jnp.inf), axis=1, keepdims=True))
            weights = settle(jnp.where(allowed, jnp.exp(scores - row_max), 0.0))
            return jnp.dot(weights, head_values, precision=lax.Precision.HIGHEST)
        blocks = lax.map(one_block, jnp.arange(SEQUENCE_TOKENS // query_span, dtype=jnp.int32))
        return blocks.reshape(SEQUENCE_TOKENS, HEAD_DIM)
    attended = lax.map(one_head, jnp.arange(ATTENTION_HEADS, dtype=jnp.int32))
    attended = jnp.transpose(attended, (1, 0, 2)).reshape(SEQUENCE_TOKENS, ATTN_WIDTH)
    attn_mixed = head_norm(attended, HEAD_DIM, attn_out_gain).astype(jnp.bfloat16)
    gated = settle(project(inner_gate_weight) * project(conv_input_weight))
    padded = jnp.concatenate([jnp.zeros((CONV_K - 1, CONV_WIDTH), jnp.float32), gated], axis=0)
    convolved = conv_taps[0] * padded[0:SEQUENCE_TOKENS]
    for tap_index in range(1, CONV_K):
        convolved = convolved + conv_taps[tap_index] * padded[tap_index:tap_index + SEQUENCE_TOKENS]
    conv_mixed = head_norm(project(outer_gate_weight) * convolved, HEAD_DIM, conv_out_gain).astype(jnp.bfloat16)
    attn_slice = ATTN_WIDTH // N_TP
    conv_slice = CONV_WIDTH // N_TP
    total = jnp.zeros((SEQUENCE_TOKENS, D), jnp.float32)
    for slice_index in range(N_TP):
        attn_lo = slice_index * attn_slice
        conv_lo = slice_index * conv_slice
        partial_value = jnp.dot(attn_mixed[:, attn_lo:attn_lo + attn_slice], attn_out_weight[attn_lo:attn_lo + attn_slice], preferred_element_type=jnp.float32)
        partial_value = partial_value + jnp.dot(conv_mixed[:, conv_lo:conv_lo + conv_slice], conv_out_weight[conv_lo:conv_lo + conv_slice], preferred_element_type=jnp.float32)
        total = total + settle(partial_value)
    return total.astype(jnp.bfloat16)
```

```python
import functools
import math

import jax
import jax.numpy as jnp
from jax import lax
from jax.experimental import pallas as pl
from jax.experimental.pallas import tpu as pltpu
from jax.sharding import PartitionSpec as P

NORM_EPSILON = 1e-06
MESH = pl.DeviceIdType.MESH
VMEM = pltpu.VMEM
LOG2E = math.log2(math.e)
ROWS = 1024
HEAD = 64
QROWS = 80
KVROWS = 144
TILE = 512
F32 = jnp.float32
BF16 = jnp.bfloat16


def attend_kernel(
    q_ref, kv_ref, gain_ref, out_ref,
    qbuf, kvbuf, gbuf, kaug, s_ref, m_ref, acc_ref, stage,
    zsend, ysend, dsend, osend, qrecv, kvrecv, grecv, orecv,
):
    sp = lax.axis_index("sp")
    tp = lax.axis_index("tp")
    z, y = sp // 4, sp % 4
    c = tp % 2
    chip = tp - c
    zc = jnp.where((z == 1) | (z == 2), 1, 0)
    set_a = c
    set_b = 3 - c

    def dev(zz, yy, cc):
        return {"sp": zz * 4 + yy, "tp": chip + cc}

    barrier = pltpu.get_barrier_semaphore()
    for step in range(1, 8):
        other = (z * 2 + c + step) % 8
        pl.semaphore_signal(
            barrier, inc=1, device_id=dev(other // 2, y, other % 2), device_id_type=MESH
        )
    for step in (1, 3):
        pl.semaphore_signal(
            barrier, inc=1, device_id=dev(z, (y + step) % 4, c), device_id_type=MESH
        )
    pl.semaphore_wait(barrier, 9)

    qslot = z // 2
    for i in range(2):
        zt = 2 * c + i
        own = (zt == z) & (zc == c)
        pieces = (
            (kv_ref.at[i], kvbuf.at[sp], kvrecv.at[sp]),
            (q_ref.at[i], qbuf.at[qslot, pl.ds(0, QROWS)], qrecv.at[qslot]),
            (gain_ref.at[i], gbuf.at[qslot], grecv.at[qslot]),
        )

        @pl.when(own)
        def _():
            for src, dst, recv in pieces:
                pltpu.make_async_copy(src, dst, recv).start()

        @pl.when(jnp.logical_not(own))
        def _():
            for n, (src, dst, recv) in enumerate(pieces):
                pltpu.make_async_remote_copy(
                    src_ref=src, dst_ref=dst, send_sem=zsend.at[i, n], recv_sem=recv,
                    device_id=dev(zt, y, zc), device_id_type=MESH,
                ).start()

    for slot in range(2):
        qbuf[slot, QROWS:, :] = jnp.zeros((128 - QROWS, ROWS), BF16)
    m_ref[...] = jnp.full_like(m_ref, -1e30)
    acc_ref[...] = jnp.zeros_like(acc_ref)

    def arrived(b):
        pltpu.make_async_copy(kvbuf.at[b], kvbuf.at[b], kvrecv.at[b]).wait()

    def along(n, b, yy):
        pltpu.make_async_remote_copy(
            src_ref=kvbuf.at[b], dst_ref=kvbuf.at[b], send_sem=ysend.at[n],
            recv_sem=kvrecv.at[b], device_id=dev(z, yy, c), device_id_type=MESH,
        ).start()

    def across(n, b):
        pltpu.make_async_remote_copy(
            src_ref=kvbuf.at[b], dst_ref=kvbuf.at[b], send_sem=dsend.at[n],
            recv_sem=kvrecv.at[b], device_id=dev(z, y, 1 - c), device_id_type=MESH,
        ).start()

    up, down, far = (y + 1) % 4, (y + 3) % 4, (y + 2) % 4

    def share(k, ys):
        across(k, set_a * 4 + ys)

        @pl.when(c == 1)
        def _():
            across(4 + k, set_b * 4 + ys)

    own_a, own_b = set_a * 4 + y, set_b * 4 + y
    arrived(own_a)
    along(0, own_a, up)
    across(0, own_a)
    arrived(own_b)
    along(1, own_b, down)
    along(2, own_b, up)
    along(3, own_a, down)

    @pl.when(c == 1)
    def _():
        across(4, own_b)

    for slot in range(2):
        pltpu.make_async_copy(
            qbuf.at[slot, pl.ds(0, QROWS)], qbuf.at[slot, pl.ds(0, QROWS)], qrecv.at[slot]
        ).wait()
        pltpu.make_async_copy(gbuf.at[slot], gbuf.at[slot], grecv.at[slot]).wait()

    def lay_keys(b, slot):
        block = jnp.concatenate(
            [kvbuf[b, HEAD:, :], jnp.zeros((128 - QROWS, ROWS), BF16)], axis=0
        )
        kaug[slot] = block.T

    def fold(qs, b, s, tile, keys):
        at = pl.ds(tile * TILE, TILE)
        old = m_ref[qs, :, at]
        new = jnp.maximum(old, jnp.max(s, axis=0, keepdims=True))
        p = jnp.exp2(s - new).astype(BF16)
        factor = jnp.exp2(old - new)
        acc_ref[qs, :, at] = acc_ref[qs, :, at] * factor + jnp.dot(
            kvbuf[b, 0:HEAD, 0:keys], p, preferred_element_type=F32
        )
        m_ref[qs, :, at] = new

    def scores(slot, qs, tile, keys=ROWS):
        return jnp.dot(
            kaug[slot, 0:keys, :], qbuf[qs, :, pl.ds(tile * TILE, TILE)],
            preferred_element_type=F32,
        )

    def masked(s, keys):
        key = lax.broadcasted_iota(jnp.int32, (TILE, TILE), 0)
        query = lax.broadcasted_iota(jnp.int32, (TILE, TILE), 1)
        last = jnp.where(key <= query, s[keys - TILE :, :], -1e30)
        if keys == TILE:
            return last
        return jnp.concatenate([s[: keys - TILE, :], last], axis=0)

    def diagonal(n, carry):
        b = jnp.where(n == 0, own_a, own_b)
        lay_keys(b, 0)
        for tile in range(2):
            keys = (tile + 1) * TILE
            fold(n, b, masked(scores(0, n, tile, keys), keys), tile, keys)
        return carry

    lax.fori_loop(0, 2, diagonal, 0)

    def group(ys, count):
        def item(n):
            qs = jnp.where(n < 3, jnp.where((c == 1) & (n == 0), 0, 1), n - 3)
            always = jnp.where(c == 0, n, n // 2)
            zs = jnp.where(n < 3, always, jnp.where(n == 3, set_a, set_b))
            return qs, zs * 4 + ys

        qs, b = item(0)
        lay_keys(b, 0)
        s_ref[0] = scores(0, qs, 0)

        def body(n, carry):
            qs, b = item(n)
            qn, bn = item(jnp.minimum(n + 1, count - 1))
            cur = n % 2
            s_ref[1] = scores(cur, qs, 1)
            fold(qs, b, s_ref[0], 0, ROWS)
            lay_keys(bn, 1 - cur)
            s_ref[0] = scores(1 - cur, qn, 0)
            fold(qs, b, s_ref[1], 1, ROWS)
            return carry

        lax.fori_loop(0, count, body, 0)

    def shared_arrived(ys):
        @pl.when(c == 0)
        def _():
            arrived(4 + ys)
            arrived(8 + ys)

        @pl.when(c == 1)
        def _():
            arrived(ys)

    shared_arrived(y)
    group(y, 3)

    arrived(set_a * 4 + down)
    along(4, set_a * 4 + down, up)
    arrived(set_b * 4 + up)
    along(5, set_b * 4 + up, down)
    arrived(set_b * 4 + down)
    share(1, down)
    arrived(set_a * 4 + up)
    share(2, up)
    shared_arrived(down)
    group(down, jnp.where(down < y, 5, 3))
    arrived(set_a * 4 + far)
    arrived(set_b * 4 + far)
    share(3, far)
    shared_arrived(up)
    group(up, jnp.where(up < y, 5, 3))
    shared_arrived(far)
    group(far, jnp.where(far < y, 5, 3))

    for slot in range(2):
        acc = acc_ref[slot]
        scale = lax.rsqrt(jnp.mean(acc * acc, axis=0, keepdims=True) + NORM_EPSILON)
        stage[slot] = (acc * scale * gbuf[slot][:, 0:1]).astype(BF16)

    half = pl.ds(pl.multiple_of((z % 2) * HEAD, HEAD), HEAD)
    for slot in range(2):
        zt = jnp.where(slot == 0, set_a, set_b)
        own = (zt == z) & (z // 2 == c)
        dst, recv = out_ref.at[half], orecv.at[z % 2]

        @pl.when(own)
        def _():
            pltpu.make_async_copy(stage.at[slot], dst, recv).start()

        @pl.when(jnp.logical_not(own))
        def _():
            pltpu.make_async_remote_copy(
                src_ref=stage.at[slot], dst_ref=dst, send_sem=osend.at[slot], recv_sem=recv,
                device_id=dev(zt, y, z // 2), device_id_type=MESH,
            ).start()

    for i in range(2):
        zt = 2 * c + i
        own = (zt == z) & (zc == c)

        @pl.when(jnp.logical_not(own))
        def _():
            for n, src in enumerate((kv_ref.at[i], q_ref.at[i], gain_ref.at[i])):
                pltpu.make_async_copy(src, src, zsend.at[i, n]).wait()

    for n in range(6):
        pltpu.make_async_copy(kvbuf.at[0], kvbuf.at[0], ysend.at[n]).wait()
    for n in range(4):
        pltpu.make_async_copy(kvbuf.at[0], kvbuf.at[0], dsend.at[n]).wait()

    @pl.when(c == 1)
    def _():
        for n in range(4, 8):
            pltpu.make_async_copy(kvbuf.at[0], kvbuf.at[0], dsend.at[n]).wait()

    for slot in range(2):
        zt = jnp.where(slot == 0, set_a, set_b)
        own = (zt == z) & (z // 2 == c)

        @pl.when(jnp.logical_not(own))
        def _():
            pltpu.make_async_copy(stage.at[slot], stage.at[slot], osend.at[slot]).wait()

        piece = out_ref.at[pl.ds(slot * HEAD, HEAD)]
        pltpu.make_async_copy(piece, piece, orecv.at[slot]).wait()


def attend(q, kv, gain):
    DMA = pltpu.SemaphoreType.DMA
    return pl.pallas_call(
        attend_kernel,
        out_shape=jax.ShapeDtypeStruct((2 * HEAD, ROWS), BF16),
        in_specs=[pl.BlockSpec(memory_space=VMEM)] * 3,
        out_specs=pl.BlockSpec(memory_space=VMEM),
        scratch_shapes=[
            VMEM((2, 128, ROWS), BF16),
            VMEM((16, KVROWS, ROWS), BF16),
            VMEM((2, HEAD, 128), F32),
            VMEM((2, ROWS, 128), BF16),
            VMEM((2, ROWS, TILE), F32),
            VMEM((2, 1, ROWS), F32),
            VMEM((2, HEAD, ROWS), F32),
            VMEM((2, HEAD, ROWS), BF16),
            DMA((2, 3)), DMA((6,)), DMA((8,)), DMA((2,)),
            DMA((2,)), DMA((16,)), DMA((2,)), DMA((2,)),
        ],
        compiler_params=pltpu.CompilerParams(
            collective_id=1, has_side_effects=True, vmem_limit_bytes=40 * 2**20
        ),
        name="attend",
    )(q, kv, gain)


def three_parts(g):
    hi = lax.reduce_precision(g, 8, 7)
    mid = lax.reduce_precision(g - hi, 8, 7)
    low = g - hi - mid
    return jnp.stack([hi, mid, low], axis=1)


def shifted(shard, axis, by):
    devices = lax.axis_size(axis)
    pairs = [(i, i + by) for i in range(devices) if 0 <= i + by < devices]
    return lax.ppermute(shard, axis, pairs)


def norm_t(values, gain):
    grouped = values.reshape(-1, HEAD, values.shape[1])
    normed = grouped * lax.rsqrt(
        jnp.mean(grouped * grouped, axis=1, keepdims=True) + NORM_EPSILON
    )
    return normed * gain.reshape(-1, HEAD, 1)


def per_device(
    tokens, mix_gain, query_weight, key_weight, value_weight, outer_gate_weight,
    inner_gate_weight, conv_input_weight, query_gain, key_gain, gate_totals, conv_taps,
    attn_out_gain, conv_out_gain, attn_out_weight, conv_out_weight,
):
    stacked = jnp.concatenate(
        [query_weight, key_weight, value_weight, outer_gate_weight, inner_gate_weight,
         conv_input_weight], axis=1,
    )
    gathered = lax.all_gather(tokens, "tp", axis=1, tiled=True).astype(F32)
    squares = jnp.sum(gathered * gathered, axis=1)
    scaled = (gathered * mix_gain).astype(BF16)
    row_scale = lax.rsqrt(squares / mix_gain.shape[0] + NORM_EPSILON)
    projected = lax.dot_general(
        stacked, scaled, (((0,), (1,)), ((), ())), preferred_element_type=F32
    ) * row_scale[None, :]
    pq, pk, pv, po, pi, px = [projected[n * 128 : (n + 1) * 128] for n in range(6)]
    factor = LOG2E * HEAD**-0.5
    queries = norm_t(pq, jnp.tile(query_gain, 2) * factor)
    keys = norm_t(pk, jnp.tile(key_gain, 2))
    parts = three_parts(gate_totals.T * LOG2E)
    ones = jnp.ones_like(parts)
    none = jnp.zeros((2, 10, ROWS), F32)
    q = jnp.concatenate([queries, ones, parts, none], axis=1).astype(BF16)
    kv = jnp.concatenate(
        [pv.reshape(2, HEAD, ROWS), keys, -parts, ones, none], axis=1
    ).astype(BF16)
    gain = jnp.broadcast_to(attn_out_gain.reshape(2, HEAD, 1), (2, HEAD, 128))
    attn_mixed = attend(q, kv, gain)

    gated = (pi * px).astype(BF16)
    prior = shifted(gated[:, ROWS - 2 :], "sp", 1)
    padded = jnp.concatenate([prior, gated], axis=1).astype(F32)
    convolved = conv_taps[0][:, None] * padded[:, 0:ROWS]
    for tap in range(1, 3):
        convolved = convolved + conv_taps[tap][:, None] * padded[:, tap : tap + ROWS]
    conv_mixed = norm_t(po * convolved, conv_out_gain).reshape(128, ROWS).astype(BF16)
    joined = jnp.concatenate([attn_mixed, conv_mixed], axis=0)
    out_weight = jnp.concatenate([attn_out_weight, conv_out_weight], axis=0)
    return lax.psum_scatter(
        lax.dot_general(
            joined, out_weight, (((0,), (0,)), ((), ())), preferred_element_type=F32
        ).astype(BF16),
        "tp", scatter_dimension=0, tiled=True,
    )


def solution(mesh):
    placed = (
        P("sp", "tp"), P(), P(None, "tp"), P(None, "tp"), P(None, "tp"), P(None, "tp"),
        P(None, "tp"), P(None, "tp"), P(), P(), P("sp", "tp"), P(None, "tp"), P("tp"),
        P("tp"), P("tp", None), P("tp", None),
    )
    return jax.shard_map(
        per_device, mesh=mesh, in_specs=placed, out_specs=P(("sp", "tp"), None), check_vma=False
    )
```

```python
import math

import jax
import jax.numpy as jnp
from jax import lax
from jax.experimental import pallas as pl
from jax.experimental.pallas import tpu as pltpu
from jax.sharding import PartitionSpec as P

NORM_EPSILON = 1e-06
MESH = pl.DeviceIdType.MESH
VMEM = pltpu.VMEM
LOG2E = math.log2(math.e)
WIDTH = 2048
ROWS = 1024
CHUNK = 256
FEATURES = 256
HEAD = 64
QROWS = 80
KVROWS = 144
TILE = 512
F32 = jnp.float32
BF16 = jnp.bfloat16


def column(row):
    return jnp.broadcast_to(row, (128, 128)).T


def norm_rows(values, gain):
    scale = lax.rsqrt(jnp.mean(values * values, axis=0, keepdims=True) + NORM_EPSILON)
    return values * scale * gain


def layer_kernel(
    tokens, mix, wq, wk, wv, wo, wi, wx, qgain, kgain, gates, taps, again, cgain, wa, wc,
    out_ref,
    xbuf, wtmp, wt, xs, proj, outer, gated, halo, qout, kvout, gout, cols,
    qbuf, kvbuf, gbuf, kaug, s_ref, m_ref, acc_ref, stage, cstage, wbuf, cbuf, oacc,
    lsem, xsend, xdsend, xrecv, hsem, zsend, gsend, ysend, dsend, osend, csend, wsend,
    qrecv, kvrecv, grecv, wrecv, arecv, crecv,
):
    sp = lax.axis_index("sp")
    tp = lax.axis_index("tp")
    z, y = sp // 4, sp % 4
    x, c = tp // 2, tp % 2
    zc = jnp.where((z == 1) | (z == 2), 1, 0)
    set_a = c
    set_b = 3 - c

    def dev(zz, yy, xx, cc):
        return {"sp": zz * 4 + yy, "tp": xx * 2 + cc}

    def local(src, dst, sem):
        return pltpu.make_async_copy(src, dst, sem)

    def remote(src, dst, send, recv, to):
        return pltpu.make_async_remote_copy(
            src_ref=src, dst_ref=dst, send_sem=send, recv_sem=recv, device_id=to,
            device_id_type=MESH,
        )

    def drain(ref, sem):
        pltpu.make_async_copy(ref, ref, sem).wait()

    mine = local(tokens, xbuf.at[tp], lsem.at[0])
    mine.start()
    weights = [
        local(w, wtmp.at[n], lsem.at[1 + n]) for n, w in enumerate((wq, wk, wv, wo, wi, wx))
    ]
    for w in weights:
        w.start()
    own_wa = pl.ds(pl.multiple_of(tp * 128, 128), 128)
    own_wc = pl.ds(pl.multiple_of(1024 + tp * 128, 128), 128)
    out_a = local(wa, wbuf.at[own_wa], lsem.at[7])
    out_c = local(wc, wbuf.at[own_wc], lsem.at[8])
    out_a.start()
    out_c.start()

    barrier = pltpu.get_barrier_semaphore()

    def greet(step, carry):
        other = (z * 8 + tp + step) % 32
        pl.semaphore_signal(
            barrier, inc=1, device_id={"sp": (other // 8) * 4 + y, "tp": other % 8},
            device_id_type=MESH,
        )
        return carry

    lax.fori_loop(1, 32, greet, 0)
    for step in (1, 3):
        pl.semaphore_signal(
            barrier, inc=1, device_id=dev(z, (y + step) % 4, x, c), device_id_type=MESH
        )
    for step in (1, 15):
        pl.semaphore_signal(
            barrier, inc=1, device_id={"sp": (sp + step) % 16, "tp": tp}, device_id_type=MESH
        )
    mine.wait()
    pl.semaphore_wait(barrier, 35)

    right, left, across_x = (x + 1) % 4, (x + 3) % 4, (x + 2) % 4
    sib = dev(z, y, x, 1 - c)

    def rows(t, n, half=None):
        if half is None:
            return xbuf.at[t, pl.ds(pl.multiple_of(n * CHUNK, CHUNK), CHUNK)]
        return xbuf.at[t, pl.ds(pl.multiple_of(n * CHUNK + half * 128, 128), 128)]

    def send_own(n):
        piece = rows(tp, n)
        remote(piece, piece, xsend.at[0, n], xrecv.at[tp, n], dev(z, y, right, c)).start()
        remote(piece, piece, xsend.at[1, n], xrecv.at[tp, n], dev(z, y, left, c)).start()
        remote(piece, piece, xdsend.at[0, n], xrecv.at[tp, n], sib).start()

    send_own(0)
    send_own(1)

    for n, row in enumerate((qgain, kgain)):
        both = jnp.concatenate([row[...], row[...]], axis=1)
        if n == 0:
            both = both * (LOG2E * HEAD**-0.5)
        cols[n] = column(both)
    for n in range(3):
        cols[2 + n] = column(taps[n : n + 1, :])
    cols[5] = column(cgain[...])
    out_gain = column(again[...])
    for i in range(2):
        gout[i] = out_gain[i * HEAD : (i + 1) * HEAD]
    spot = lax.broadcasted_iota(jnp.int32, (16, ROWS), 0)
    for i in range(2):
        g = gates[i : i + 1, :] * LOG2E
        hi = g.astype(BF16).astype(F32)
        mid = (g - hi).astype(BF16).astype(F32)
        low = g - hi - mid
        one = jnp.where(spot < 3, 1.0, 0.0)
        parts = jnp.where(spot == 3, hi, jnp.where(spot == 4, mid, jnp.where(spot == 5, low, one)))
        qout[i, HEAD:, :] = parts.astype(BF16)
        one = jnp.where((spot > 2) & (spot < 6), 1.0, 0.0)
        parts = jnp.where(spot == 0, -hi, jnp.where(spot == 1, -mid, jnp.where(spot == 2, -low, one)))
        kvout[i, 2 * HEAD :, :] = parts.astype(BF16)
    for n, w in enumerate(weights):
        w.wait()
        for k in range(4):
            wt[n * 128 : (n + 1) * 128, k * 512 : (k + 1) * 512] = wtmp[
                n, k * 512 : (k + 1) * 512, :
            ].T

    for slot in range(2):
        qbuf[slot, QROWS:, :] = jnp.zeros((128 - QROWS, ROWS), BF16)
    m_ref[...] = jnp.full_like(m_ref, -1e30)
    acc_ref[...] = jnp.zeros_like(acc_ref)

    @pl.when(sp == 0)
    def _():
        halo[...] = jnp.zeros_like(halo)

    qslot = z // 2

    def z_sends(n):
        at = pl.ds(pl.multiple_of(n * CHUNK, CHUNK), CHUNK)
        for i in range(2):
            zt = 2 * c + i
            own = (zt == z) & (zc == c)
            pieces = (
                (kvout.at[i, :, at], kvbuf.at[sp, :, at], kvrecv.at[sp]),
                (qout.at[i, :, at], qbuf.at[qslot, pl.ds(0, QROWS), at], qrecv.at[qslot]),
            )

            @pl.when(own)
            def _():
                for src, dst, recv in pieces:
                    local(src, dst, recv).start()

            @pl.when(jnp.logical_not(own))
            def _():
                for k, (src, dst, recv) in enumerate(pieces):
                    remote(src, dst, zsend.at[i, k, n], recv, dev(zt, y, x, zc)).start()

    for i in range(2):
        zt = 2 * c + i
        own = (zt == z) & (zc == c)

        @pl.when(own)
        def _():
            local(gout.at[i], gbuf.at[qslot], grecv.at[qslot]).start()

        @pl.when(jnp.logical_not(own))
        def _():
            remote(
                gout.at[i], gbuf.at[qslot], gsend.at[i], grecv.at[qslot], dev(zt, y, x, zc)
            ).start()

    def project(n):
        at = pl.ds(pl.multiple_of(n * CHUNK, CHUNK), CHUNK)
        squares = jnp.zeros((CHUNK, 128), F32)
        for t in range(8):
            piece = xbuf[t, at, :].astype(F32)
            squares = squares + piece[:, :128] * piece[:, :128] + piece[:, 128:] * piece[:, 128:]
            lanes = slice(t * FEATURES, (t + 1) * FEATURES)
            xs[:, lanes] = (piece * mix[:, lanes]).astype(BF16)
        total = jnp.sum(squares.T, axis=0, keepdims=True)
        row_scale = lax.rsqrt(total / WIDTH + NORM_EPSILON)
        proj[...] = lax.dot_general(
            wt[...], xs[...], (((1,), (1,)), ((), ())), preferred_element_type=F32
        ) * row_scale
        for i in range(2):
            lo = i * HEAD
            wide = [
                jnp.concatenate([cols[k, lo : lo + HEAD]] * 2, axis=1) for k in range(2)
            ]
            qout[i, 0:HEAD, at] = norm_rows(proj[lo : lo + HEAD], wide[0]).astype(BF16)
            kvout[i, HEAD : 2 * HEAD, at] = norm_rows(
                proj[128 + lo : 128 + lo + HEAD], wide[1]
            ).astype(BF16)
            kvout[i, 0:HEAD, at] = proj[256 + lo : 256 + lo + HEAD].astype(BF16)
        outer[:, at] = proj[384:512]
        gated[:, at] = (proj[512:640] * proj[640:768]).astype(BF16)

    def gather(n, carry):
        @pl.when(n < 4)
        def _():
            before, after = left * 2 + c, right * 2 + c
            drain(rows(before, n), xrecv.at[before, n])
            piece = rows(before, n, 0)
            remote(piece, piece, xsend.at[2, n], xrecv.at[before, n], dev(z, y, right, c)).start()
            piece = rows(before, n)
            remote(piece, piece, xdsend.at[1, n], xrecv.at[before, n], sib).start()
            drain(rows(after, n), xrecv.at[after, n])
            piece = rows(after, n, 1)
            remote(piece, piece, xsend.at[3, n], xrecv.at[after, n], dev(z, y, left, c)).start()
            piece = rows(after, n)
            remote(piece, piece, xdsend.at[2, n], xrecv.at[after, n], sib).start()

            @pl.when(n < 2)
            def _():
                send_own(n + 2)

        @pl.when(n > 0)
        def _():
            done = n - 1
            far = across_x * 2 + c
            drain(rows(far, done), xrecv.at[far, done])
            piece = rows(far, done)
            remote(piece, piece, xdsend.at[3, done], xrecv.at[far, done], sib).start()
            for xx in range(4):
                t = xx * 2 + 1 - c
                drain(rows(t, done), xrecv.at[t, done])
            project(done)
            z_sends(done)

        return carry

    lax.fori_loop(0, 5, gather, 0)

    @pl.when(sp < 15)
    def _():
        remote(
            gated.at[:, pl.ds(ROWS - 128, 128)], halo, hsem.at[0], hsem.at[1],
            {"sp": jnp.minimum(sp + 1, 15), "tp": tp},
        ).start()

    def w_rows(t, kind):
        return pl.ds(pl.multiple_of(kind * 1024 + t * 128, 128), 128)

    def w_send(n, t, kind, to):
        piece = wbuf.at[w_rows(t, kind)]
        remote(piece, piece, wsend.at[n], wrecv.at[kind * 8 + t], to).start()

    def w_wait(t, kind):
        drain(wbuf.at[w_rows(t, kind)], wrecv.at[kind * 8 + t])

    out_a.wait()
    out_c.wait()
    w_send(0, tp, 0, dev(z, y, right, c))
    w_send(1, tp, 1, dev(z, y, left, c))
    w_send(2, tp, 1, dev(z, y, right, c))
    w_send(3, tp, 0, dev(z, y, left, c))
    w_send(4, tp, 0, sib)
    w_send(5, tp, 1, sib)

    def mix_conv():
        prior = jnp.concatenate([halo[...], gated[...]], axis=1).astype(F32)
        conv = jnp.concatenate([cols[4]] * 8, axis=1) * prior[:, 128:]
        for tap in range(2):
            moved = pltpu.roll(prior, 2 - tap, axis=1)
            conv = conv + jnp.concatenate([cols[2 + tap]] * 8, axis=1) * moved[:, 128:]
        value = outer[...] * conv
        for i in range(2):
            part = slice(i * HEAD, (i + 1) * HEAD)
            wide = jnp.concatenate([cols[5, part]] * 8, axis=1)
            cstage[part, :] = norm_rows(value[part], wide).astype(BF16)

    @pl.when(sp > 0)
    def _():
        drain(halo, hsem.at[1])

    mix_conv()
    to_rows = pl.ds(pl.multiple_of(1024 + tp * 128, 128), 128)
    local(
        cstage.at[:, pl.ds(pl.multiple_of(tp * 128, 128), 128)], cbuf.at[to_rows], crecv.at[tp]
    ).start()
    for step in range(1, 8):
        t = (tp + step) % 8
        remote(
            cstage.at[:, pl.ds(pl.multiple_of(t * 128, 128), 128)], cbuf.at[to_rows],
            csend.at[step], crecv.at[tp], {"sp": sp, "tp": t},
        ).start()

    def arrived(b):
        pltpu.make_async_copy(kvbuf.at[b], kvbuf.at[b], kvrecv.at[b]).wait()

    def along(n, b, yy):
        pltpu.make_async_remote_copy(
            src_ref=kvbuf.at[b], dst_ref=kvbuf.at[b], send_sem=ysend.at[n],
            recv_sem=kvrecv.at[b], device_id=dev(z, yy, x, c), device_id_type=MESH,
        ).start()

    def across(n, b):
        pltpu.make_async_remote_copy(
            src_ref=kvbuf.at[b], dst_ref=kvbuf.at[b], send_sem=dsend.at[n],
            recv_sem=kvrecv.at[b], device_id=sib, device_id_type=MESH,
        ).start()

    up, down, far = (y + 1) % 4, (y + 3) % 4, (y + 2) % 4

    def share(k, ys):
        across(k, set_a * 4 + ys)

        @pl.when(c == 1)
        def _():
            across(4 + k, set_b * 4 + ys)

    own_a, own_b = set_a * 4 + y, set_b * 4 + y
    arrived(own_a)
    along(0, own_a, up)
    across(0, own_a)
    arrived(own_b)
    along(1, own_b, down)
    along(2, own_b, up)
    along(3, own_a, down)

    @pl.when(c == 1)
    def _():
        across(4, own_b)

    for slot in range(2):
        pltpu.make_async_copy(
            qbuf.at[slot, pl.ds(0, QROWS)], qbuf.at[slot, pl.ds(0, QROWS)], qrecv.at[slot]
        ).wait()
        pltpu.make_async_copy(gbuf.at[slot], gbuf.at[slot], grecv.at[slot]).wait()

    def lay_keys(b, slot):
        block = jnp.concatenate(
            [kvbuf[b, HEAD:, :], jnp.zeros((128 - QROWS, ROWS), BF16)], axis=0
        )
        kaug[slot] = block.T

    def fold(qs, b, s, tile, keys):
        at = pl.ds(tile * TILE, TILE)
        old = m_ref[qs, :, at]
        new = jnp.maximum(old, jnp.max(s, axis=0, keepdims=True))
        p = jnp.exp2(s - new).astype(BF16)
        factor = jnp.exp2(old - new)
        acc_ref[qs, :, at] = acc_ref[qs, :, at] * factor + jnp.dot(
            kvbuf[b, 0:HEAD, 0:keys], p, preferred_element_type=F32
        )
        m_ref[qs, :, at] = new

    def scores(slot, qs, tile, keys=ROWS):
        return jnp.dot(
            kaug[slot, 0:keys, :], qbuf[qs, :, pl.ds(tile * TILE, TILE)],
            preferred_element_type=F32,
        )

    def masked(s, keys):
        key = lax.broadcasted_iota(jnp.int32, (TILE, TILE), 0)
        query = lax.broadcasted_iota(jnp.int32, (TILE, TILE), 1)
        last = jnp.where(key <= query, s[keys - TILE :, :], -1e30)
        if keys == TILE:
            return last
        return jnp.concatenate([s[: keys - TILE, :], last], axis=0)

    def diagonal(n, carry):
        b = jnp.where(n == 0, own_a, own_b)
        lay_keys(b, 0)
        for tile in range(2):
            keys = (tile + 1) * TILE
            fold(n, b, masked(scores(0, n, tile, keys), keys), tile, keys)
        return carry

    lax.fori_loop(0, 2, diagonal, 0)

    def group(ys, count):
        def item(n):
            qs = jnp.where(n < 3, jnp.where((c == 1) & (n == 0), 0, 1), n - 3)
            always = jnp.where(c == 0, n, n // 2)
            zs = jnp.where(n < 3, always, jnp.where(n == 3, set_a, set_b))
            return qs, zs * 4 + ys

        qs, b = item(0)
        lay_keys(b, 0)
        s_ref[0] = scores(0, qs, 0)

        def body(n, carry):
            qs, b = item(n)
            qn, bn = item(jnp.minimum(n + 1, count - 1))
            cur = n % 2
            s_ref[1] = scores(cur, qs, 1)
            fold(qs, b, s_ref[0], 0, ROWS)
            lay_keys(bn, 1 - cur)
            s_ref[0] = scores(1 - cur, qn, 0)
            fold(qs, b, s_ref[1], 1, ROWS)
            return carry

        lax.fori_loop(0, count, body, 0)

    def shared_arrived(ys):
        @pl.when(c == 0)
        def _():
            arrived(4 + ys)
            arrived(8 + ys)

        @pl.when(c == 1)
        def _():
            arrived(ys)

    shared_arrived(y)
    group(y, 3)
    before, after, far_x = left * 2 + c, right * 2 + c, across_x * 2 + c

    arrived(set_a * 4 + down)
    along(4, set_a * 4 + down, up)
    arrived(set_b * 4 + up)
    along(5, set_b * 4 + up, down)
    arrived(set_b * 4 + down)
    share(1, down)
    arrived(set_a * 4 + up)
    share(2, up)
    shared_arrived(down)
    group(down, jnp.where(down < y, 5, 3))
    w_wait(before, 0)
    w_send(6, before, 0, dev(z, y, right, c))
    w_send(7, before, 0, sib)
    w_wait(after, 1)
    w_send(8, after, 1, dev(z, y, left, c))
    w_send(9, after, 1, sib)
    arrived(set_a * 4 + far)
    arrived(set_b * 4 + far)
    share(3, far)
    shared_arrived(up)
    group(up, jnp.where(up < y, 5, 3))
    w_wait(before, 1)
    w_send(10, before, 1, sib)
    w_wait(after, 0)
    w_send(11, after, 0, sib)
    shared_arrived(far)
    group(far, jnp.where(far < y, 5, 3))

    for slot in range(2):
        stage[slot] = norm_rows(acc_ref[slot], gbuf[slot][:, 0:1]).astype(BF16)
        head = x * 4 + z
        dst = cbuf.at[pl.ds(pl.multiple_of(head * HEAD, HEAD), HEAD)]
        zt = jnp.where(slot == 0, set_a, set_b)
        for step in range(8):
            t = (tp + step) % 8
            piece = stage.at[slot, :, pl.ds(pl.multiple_of(t * 128, 128), 128)]
            if step:
                remote(
                    piece, dst, osend.at[slot, step], arecv.at[head],
                    {"sp": zt * 4 + y, "tp": t},
                ).start()
                continue

            @pl.when(zt == z)
            def _():
                local(piece, dst, arecv.at[head]).start()

            @pl.when(zt != z)
            def _():
                remote(
                    piece, dst, osend.at[slot, step], arecv.at[head],
                    {"sp": zt * 4 + y, "tp": t},
                ).start()

    w_wait(far_x, 0)
    w_send(12, far_x, 0, sib)
    w_wait(far_x, 1)
    w_send(13, far_x, 1, sib)
    for xx in range(4):
        w_wait(xx * 2 + 1 - c, 0)
        w_wait(xx * 2 + 1 - c, 1)
    for t in range(8):
        drain(cbuf.at[pl.ds(1024 + t * 128, 128)], crecv.at[t])

    def product(lo, n):
        at = pl.ds(pl.multiple_of(n * TILE, TILE), TILE)
        return jnp.dot(
            cbuf[lo : lo + 1024, :].T, wbuf[lo : lo + 1024, at], preferred_element_type=F32
        )

    def conv_part(n, carry):
        oacc[:, pl.ds(pl.multiple_of(n * TILE, TILE), TILE)] = product(1024, n)
        return carry

    lax.fori_loop(0, WIDTH // TILE, conv_part, 0)
    for h in range(16):
        drain(cbuf.at[pl.ds(h * HEAD, HEAD)], arecv.at[h])

    def attn_part(n, carry):
        at = pl.ds(pl.multiple_of(n * TILE, TILE), TILE)
        out_ref[:, at] = (oacc[:, at] + product(0, n)).astype(BF16)
        return carry

    lax.fori_loop(0, WIDTH // TILE, attn_part, 0)

    def sent(n, carry):
        for k in range(2):
            drain(rows(tp, n), xsend.at[k, n])
            drain(rows(tp, n, 0), xsend.at[2 + k, n])
        for k in range(4):
            drain(rows(tp, n), xdsend.at[k, n])
        for i in range(2):
            zt = 2 * c + i
            own = (zt == z) & (zc == c)
            at = pl.ds(pl.multiple_of(n * CHUNK, CHUNK), CHUNK)

            @pl.when(jnp.logical_not(own))
            def _():
                drain(kvout.at[i, :, at], zsend.at[i, 0, n])
                drain(qout.at[i, :, at], zsend.at[i, 1, n])

        return carry

    lax.fori_loop(0, 4, sent, 0)
    for i in range(2):
        zt = 2 * c + i
        own = (zt == z) & (zc == c)

        @pl.when(jnp.logical_not(own))
        def _():
            drain(gout.at[i], gsend.at[i])

    @pl.when(sp < 15)
    def _():
        drain(halo, hsem.at[0])

    for n in range(6):
        drain(kvbuf.at[0], ysend.at[n])
    for n in range(4):
        drain(kvbuf.at[0], dsend.at[n])

    @pl.when(c == 1)
    def _():
        for n in range(4, 8):
            drain(kvbuf.at[0], dsend.at[n])

    for n in range(14):
        drain(wbuf.at[pl.ds(0, 128)], wsend.at[n])
    for step in range(1, 8):
        drain(cbuf.at[pl.ds(0, 128)], csend.at[step])
    for slot in range(2):
        zt = jnp.where(slot == 0, set_a, set_b)
        piece = stage.at[slot, :, pl.ds(0, 128)]
        for step in range(1, 8):
            drain(piece, osend.at[slot, step])

        @pl.when(zt != z)
        def _():
            drain(piece, osend.at[slot, 0])


def per_device(
    tokens, mix_gain, query_weight, key_weight, value_weight, outer_gate_weight,
    inner_gate_weight, conv_input_weight, query_gain, key_gain, gate_totals, conv_taps,
    attn_out_gain, conv_out_gain, attn_out_weight, conv_out_weight,
):
    DMA = pltpu.SemaphoreType.DMA
    far = pl.BlockSpec(memory_space=pl.ANY)
    near = pl.BlockSpec(memory_space=VMEM)
    return pl.pallas_call(
        layer_kernel,
        out_shape=jax.ShapeDtypeStruct((128, WIDTH), BF16),
        in_specs=[far, near] + [far] * 6 + [near] * 6 + [far] * 2,
        out_specs=near,
        scratch_shapes=[
            VMEM((8, ROWS, FEATURES), BF16),
            VMEM((6, WIDTH, 128), BF16),
            VMEM((768, WIDTH), BF16),
            VMEM((CHUNK, WIDTH), BF16),
            VMEM((768, CHUNK), F32),
            VMEM((128, ROWS), F32),
            VMEM((128, ROWS), BF16),
            VMEM((128, 128), BF16),
            VMEM((2, QROWS, ROWS), BF16),
            VMEM((2, KVROWS, ROWS), BF16),
            VMEM((2, HEAD, 128), F32),
            VMEM((6, 128, 128), F32),
            VMEM((2, 128, ROWS), BF16),
            VMEM((16, KVROWS, ROWS), BF16),
            VMEM((2, HEAD, 128), F32),
            VMEM((2, ROWS, 128), BF16),
            VMEM((2, ROWS, TILE), F32),
            VMEM((2, 1, ROWS), F32),
            VMEM((2, HEAD, ROWS), F32),
            VMEM((2, HEAD, ROWS), BF16),
            VMEM((128, ROWS), BF16),
            VMEM((WIDTH, WIDTH), BF16),
            VMEM((WIDTH, 128), BF16),
            VMEM((128, WIDTH), F32),
            DMA((9,)), DMA((4, 4)), DMA((4, 4)), DMA((8, 4)), DMA((2,)),
            DMA((2, 2, 4)), DMA((2,)), DMA((6,)), DMA((8,)), DMA((2, 8)), DMA((8,)), DMA((14,)),
            DMA((2,)), DMA((16,)), DMA((2,)), DMA((16,)), DMA((16,)), DMA((8,)),
        ],
        compiler_params=pltpu.CompilerParams(
            collective_id=1, has_side_effects=True, vmem_limit_bytes=56 * 2**20
        ),
        name="layer",
    )(
        tokens, mix_gain.reshape(1, WIDTH), query_weight, key_weight, value_weight,
        outer_gate_weight, inner_gate_weight, conv_input_weight, query_gain.reshape(1, HEAD),
        key_gain.reshape(1, HEAD), gate_totals.T, conv_taps, attn_out_gain.reshape(1, 128),
        conv_out_gain.reshape(1, 128), attn_out_weight, conv_out_weight,
    )


def solution(mesh):
    placed = (
        P("sp", "tp"), P(), P(None, "tp"), P(None, "tp"), P(None, "tp"), P(None, "tp"),
        P(None, "tp"), P(None, "tp"), P(), P(), P("sp", "tp"), P(None, "tp"), P("tp"),
        P("tp"), P("tp", None), P("tp", None),
    )
    return jax.shard_map(
        per_device, mesh=mesh, in_specs=placed, out_specs=P(("sp", "tp"), None), check_vma=False
    )
```

```python
import math

import jax
import jax.numpy as jnp
from jax import lax
from jax.experimental import pallas as pl
from jax.experimental.pallas import tpu as pltpu
from jax.sharding import PartitionSpec as P

NORM_EPSILON = 1e-06
MESH = pl.DeviceIdType.MESH
VMEM = pltpu.VMEM
LOG2E = math.log2(math.e)
WIDTH = 2048
ROWS = 1024
CHUNK = 256
FEATURES = 256
HEAD = 64
QROWS = 80
KVROWS = 144
TILE = 512
F32 = jnp.float32
BF16 = jnp.bfloat16


def column(row):
    return jnp.broadcast_to(row, (128, 128)).T


def norm_rows(values, gain):
    scale = lax.rsqrt(jnp.mean(values * values, axis=0, keepdims=True) + NORM_EPSILON)
    return values * scale * gain


def layer_kernel(
    tokens, mix, wq, wk, wv, wo, wi, wx, qgain, kgain, gates, taps, again, cgain, wa, wc,
    out_ref,
    xbuf, wtmp, wt, xs, scale_ref, proj, outer, gated, halo, qout, kvout, gout, cols,
    qbuf, kvbuf, gbuf, kaug, s_ref, m_ref, acc_ref, stage, cstage, wbuf, cbuf, ct, oacc,
    lsem, xsend, xdsend, xrecv, hsem, zsend, gsend, ysend, dsend, osend, csend, wsend, hsend,
    qrecv, kvrecv, grecv, wrecv, hrecv, arecv, crecv,
):
    sp = lax.axis_index("sp")
    tp = lax.axis_index("tp")
    z, y = sp // 4, sp % 4
    x, c = tp // 2, tp % 2
    zc = jnp.where((z == 1) | (z == 2), 1, 0)
    set_a = c
    set_b = 3 - c

    def dev(zz, yy, xx, cc):
        return {"sp": zz * 4 + yy, "tp": xx * 2 + cc}

    def local(src, dst, sem):
        return pltpu.make_async_copy(src, dst, sem)

    def remote(src, dst, send, recv, to):
        return pltpu.make_async_remote_copy(
            src_ref=src, dst_ref=dst, send_sem=send, recv_sem=recv, device_id=to,
            device_id_type=MESH,
        )

    def drain(ref, sem):
        pltpu.make_async_copy(ref, ref, sem).wait()

    mine = local(tokens, xbuf.at[tp], lsem.at[0])
    mine.start()
    weights = [
        local(w, wtmp.at[n], lsem.at[1 + n]) for n, w in enumerate((wq, wk, wv, wo, wi, wx))
    ]
    for w in weights:
        w.start()
    own_wa = pl.ds(pl.multiple_of(tp * 128, 128), 128)
    own_wc = pl.ds(pl.multiple_of(1024 + tp * 128, 128), 128)
    out_a = local(wa, wbuf.at[own_wa], lsem.at[7])
    out_c = local(wc, wbuf.at[own_wc], lsem.at[8])
    out_a.start()
    out_c.start()

    barrier = pltpu.get_barrier_semaphore()

    def greet(step, carry):
        other = (z * 8 + tp + step) % 32
        pl.semaphore_signal(
            barrier, inc=1, device_id={"sp": (other // 8) * 4 + y, "tp": other % 8},
            device_id_type=MESH,
        )
        return carry

    lax.fori_loop(1, 32, greet, 0)
    for step in (1, 3):
        pl.semaphore_signal(
            barrier, inc=1, device_id=dev(z, (y + step) % 4, x, c), device_id_type=MESH
        )
    for step in (1, 15):
        pl.semaphore_signal(
            barrier, inc=1, device_id={"sp": (sp + step) % 16, "tp": tp}, device_id_type=MESH
        )
    mine.wait()
    pl.semaphore_wait(barrier, 35)

    right, left, across_x = (x + 1) % 4, (x + 3) % 4, (x + 2) % 4
    sib = dev(z, y, x, 1 - c)

    def rows(t, n, half=None):
        if half is None:
            return xbuf.at[t, pl.ds(pl.multiple_of(n * CHUNK, CHUNK), CHUNK)]
        return xbuf.at[t, pl.ds(pl.multiple_of(n * CHUNK + half * 128, 128), 128)]

    def send_own(n):
        piece = rows(tp, n)
        remote(piece, piece, xsend.at[0, n], xrecv.at[tp, n], dev(z, y, right, c)).start()
        remote(piece, piece, xsend.at[1, n], xrecv.at[tp, n], dev(z, y, left, c)).start()
        remote(piece, piece, xdsend.at[0, n], xrecv.at[tp, n], sib).start()

    send_own(0)
    send_own(1)

    for n, row in enumerate((qgain, kgain)):
        both = jnp.concatenate([row[...], row[...]], axis=1)
        if n == 0:
            both = both * (LOG2E * HEAD**-0.5)
        cols[n] = column(both)
    for n in range(3):
        cols[2 + n] = column(taps[n : n + 1, :])
    cols[5] = column(cgain[...])
    out_gain = column(again[...])
    for i in range(2):
        gout[i] = out_gain[i * HEAD : (i + 1) * HEAD]
    spot = lax.broadcasted_iota(jnp.int32, (16, ROWS), 0)
    for i in range(2):
        g = gates[i : i + 1, :] * LOG2E
        hi = g.astype(BF16).astype(F32)
        mid = (g - hi).astype(BF16).astype(F32)
        low = g - hi - mid
        one = jnp.where(spot < 3, 1.0, 0.0)
        parts = jnp.where(spot == 3, hi, jnp.where(spot == 4, mid, jnp.where(spot == 5, low, one)))
        qout[i, HEAD:, :] = parts.astype(BF16)
        one = jnp.where((spot > 2) & (spot < 6), 1.0, 0.0)
        parts = jnp.where(spot == 0, -hi, jnp.where(spot == 1, -mid, jnp.where(spot == 2, -low, one)))
        kvout[i, 2 * HEAD :, :] = parts.astype(BF16)
    for n, w in enumerate(weights):
        w.wait()
        for k in range(4):
            wt[n * 128 : (n + 1) * 128, k * 512 : (k + 1) * 512] = wtmp[
                n, k * 512 : (k + 1) * 512, :
            ].T

    for slot in range(2):
        qbuf[slot, QROWS:, :] = jnp.zeros((128 - QROWS, ROWS), BF16)
    m_ref[...] = jnp.full_like(m_ref, -1e30)
    acc_ref[...] = jnp.zeros_like(acc_ref)

    @pl.when(sp == 0)
    def _():
        halo[...] = jnp.zeros_like(halo)

    qslot = z // 2

    def z_sends(n):
        at = pl.ds(pl.multiple_of(n * CHUNK, CHUNK), CHUNK)
        for i in range(2):
            zt = 2 * c + i
            own = (zt == z) & (zc == c)
            pieces = (
                (kvout.at[i, :, at], kvbuf.at[sp, :, at], kvrecv.at[sp, n]),
                (qout.at[i, :, at], qbuf.at[qslot, pl.ds(0, QROWS), at], qrecv.at[qslot, n]),
            )

            @pl.when(own)
            def _():
                for src, dst, recv in pieces:
                    local(src, dst, recv).start()

            @pl.when(jnp.logical_not(own))
            def _():
                for k, (src, dst, recv) in enumerate(pieces):
                    remote(src, dst, zsend.at[i, k, n], recv, dev(zt, y, x, zc)).start()

    for i in range(2):
        zt = 2 * c + i
        own = (zt == z) & (zc == c)

        @pl.when(own)
        def _():
            local(gout.at[i], gbuf.at[qslot], grecv.at[qslot]).start()

        @pl.when(jnp.logical_not(own))
        def _():
            remote(
                gout.at[i], gbuf.at[qslot], gsend.at[i], grecv.at[qslot], dev(zt, y, x, zc)
            ).start()

    def project(n):
        at = pl.ds(pl.multiple_of(n * CHUNK, CHUNK), CHUNK)
        squares = jnp.zeros((CHUNK, 128), F32)
        for t in range(8):
            piece = xbuf[t, at, :].astype(F32)
            squares = squares + piece[:, :128] * piece[:, :128] + piece[:, 128:] * piece[:, 128:]
            lanes = slice(t * FEATURES, (t + 1) * FEATURES)
            xs[:, lanes] = (piece * mix[:, lanes]).astype(BF16)
        total = jnp.sum(squares.T, axis=0, keepdims=True)
        row_scale = lax.rsqrt(total / WIDTH + NORM_EPSILON)
        scale_ref[...] = row_scale
        proj[0:384] = lax.dot_general(
            wt[0:384], xs[...], (((1,), (1,)), ((), ())), preferred_element_type=F32
        ) * row_scale
        for i in range(2):
            lo = i * HEAD
            wide = [
                jnp.concatenate([cols[k, lo : lo + HEAD]] * 2, axis=1) for k in range(2)
            ]
            qout[i, 0:HEAD, at] = norm_rows(proj[lo : lo + HEAD], wide[0]).astype(BF16)
            kvout[i, HEAD : 2 * HEAD, at] = norm_rows(
                proj[128 + lo : 128 + lo + HEAD], wide[1]
            ).astype(BF16)
            kvout[i, 0:HEAD, at] = proj[256 + lo : 256 + lo + HEAD].astype(BF16)

    def project_conv(n):
        at = pl.ds(pl.multiple_of(n * CHUNK, CHUNK), CHUNK)
        proj[384:768] = lax.dot_general(
            wt[384:768], xs[...], (((1,), (1,)), ((), ())), preferred_element_type=F32
        ) * scale_ref[...]
        outer[:, at] = proj[384:512]
        gated[:, at] = (proj[512:640] * proj[640:768]).astype(BF16)

    def chunk(b, k):
        return kvbuf.at[b, :, pl.ds(pl.multiple_of(k * CHUNK, CHUNK), CHUNK)]

    def arrived(b, k):
        drain(chunk(b, k), kvrecv.at[b, k])

    def along(n, b, k, yy):
        piece = chunk(b, k)
        remote(piece, piece, ysend.at[n, k], kvrecv.at[b, k], dev(z, yy, x, c)).start()

    def across(n, b, k):
        piece = chunk(b, k)
        remote(piece, piece, dsend.at[n, k], kvrecv.at[b, k], sib).start()

    up, down, far = (y + 1) % 4, (y + 3) % 4, (y + 2) % 4
    own_a, own_b = set_a * 4 + y, set_b * 4 + y

    def share_a(n, ys, k):
        across(n, set_a * 4 + ys, k)

    def share_b(n, ys, k):
        @pl.when(c == 1)
        def _():
            across(4 + n, set_b * 4 + ys, k)

    def first_hop(k):
        arrived(own_a, k)
        along(0, own_a, k, up)
        arrived(own_b, k)
        along(1, own_b, k, down)
        along(2, own_b, k, up)
        along(3, own_a, k, down)
        share_a(0, y, k)
        share_b(0, y, k)

    def second_hop(k):
        arrived(set_a * 4 + down, k)
        along(4, set_a * 4 + down, k, up)
        arrived(set_b * 4 + up, k)
        along(5, set_b * 4 + up, k, down)
        share_a(1, down, k)
        share_b(2, up, k)
        arrived(set_b * 4 + down, k)
        share_b(1, down, k)
        arrived(set_a * 4 + up, k)
        share_a(2, up, k)

    def last_hop(k):
        arrived(set_a * 4 + far, k)
        share_a(3, far, k)
        arrived(set_b * 4 + far, k)
        share_b(3, far, k)

    def shared_arrived(ys):
        @pl.when(c == 0)
        def _():
            for k in range(4):
                arrived(4 + ys, k)
                arrived(8 + ys, k)

        @pl.when(c == 1)
        def _():
            for k in range(4):
                arrived(ys, k)

    def w_rows(t, kind):
        return pl.ds(pl.multiple_of(kind * 1024 + t * 128, 128), 128)

    def w_send(n, t, kind, to):
        piece = wbuf.at[w_rows(t, kind)]
        remote(piece, piece, wsend.at[n], wrecv.at[kind * 8 + t], to).start()

    def w_wait(t, kind):
        drain(wbuf.at[w_rows(t, kind)], wrecv.at[kind * 8 + t])

    before, after, far_x = left * 2 + c, right * 2 + c, across_x * 2 + c
    near_z = z + 1 - 2 * (z % 2)

    def h_rows(t, half):
        return wbuf.at[pl.ds(pl.multiple_of(1024 + t * 128 + half * 64, 64), 64)]

    def h_send(n, t, to):
        piece = h_rows(t, z % 2)
        remote(piece, piece, hsend.at[n], hrecv.at[t, z % 2], to).start()

    def h_wait(t, half):
        drain(h_rows(t, half), hrecv.at[t, half])

    def w_first():
        out_a.wait()
        out_c.wait()
        h_send(0, tp, dev(z, y, right, c))
        h_send(1, tp, dev(z, y, left, c))
        w_send(2, tp, 0, sib)
        w_send(3, tp, 1, sib)

    def w_second():
        h_wait(before, z % 2)
        h_wait(after, z % 2)

        @pl.when(c == 0)
        def _():
            h_send(2, before, dev(z, y, right, c))

        @pl.when(c == 1)
        def _():
            h_send(2, after, dev(z, y, left, c))

        w_send(0, tp, 0, dev(z, y, right, c))
        w_send(1, tp, 0, dev(z, y, left, c))

    def w_third():
        partner = dev(near_z, y, x, c)
        h_send(3, before, partner)
        h_send(4, after, partner)

    def w_far():
        h_wait(far_x, z % 2)
        h_send(5, far_x, dev(near_z, y, x, c))

    def w_fourth():
        w_wait(before, 0)
        w_wait(after, 0)

        @pl.when(c == 0)
        def _():
            w_send(4, before, 0, dev(z, y, right, c))

        @pl.when(c == 1)
        def _():
            w_send(4, after, 0, dev(z, y, left, c))

        w_send(5, before, 0, sib)
        w_send(6, after, 0, sib)

    def w_fifth():
        for n, t in enumerate((before, after, far_x)):
            h_wait(t, 1 - z % 2)
            w_send(7 + n, t, 1, sib)

    def gather(n, carry):
        @pl.when(n < 4)
        def _():
            drain(rows(before, n), xrecv.at[before, n])
            piece = rows(before, n, 0)
            remote(piece, piece, xsend.at[2, n], xrecv.at[before, n], dev(z, y, right, c)).start()
            piece = rows(before, n)
            remote(piece, piece, xdsend.at[1, n], xrecv.at[before, n], sib).start()
            drain(rows(after, n), xrecv.at[after, n])
            piece = rows(after, n, 1)
            remote(piece, piece, xsend.at[3, n], xrecv.at[after, n], dev(z, y, left, c)).start()
            piece = rows(after, n)
            remote(piece, piece, xdsend.at[2, n], xrecv.at[after, n], sib).start()

            @pl.when(n < 2)
            def _():
                send_own(n + 2)

            @pl.when(n == 3)
            def _():
                w_first()

        @pl.when(n > 0)
        def _():
            done = n - 1
            far = across_x * 2 + c
            drain(rows(far, done), xrecv.at[far, done])
            piece = rows(far, done)
            remote(piece, piece, xdsend.at[3, done], xrecv.at[far, done], sib).start()
            for xx in range(4):
                t = xx * 2 + 1 - c
                drain(rows(t, done), xrecv.at[t, done])
            project(done)
            z_sends(done)
            project_conv(done)

        @pl.when((n > 1) & (n < 4))
        def _():
            first_hop(n - 2)

        @pl.when(n == 3)
        def _():
            second_hop(n - 3)

        return carry

    lax.fori_loop(0, 5, gather, 0)

    @pl.when(sp < 15)
    def _():
        remote(
            gated.at[:, pl.ds(ROWS - 128, 128)], halo, hsem.at[0], hsem.at[1],
            {"sp": jnp.minimum(sp + 1, 15), "tp": tp},
        ).start()

    def mix_conv():
        prior = jnp.concatenate([halo[...], gated[...]], axis=1).astype(F32)
        conv = jnp.concatenate([cols[4]] * 8, axis=1) * prior[:, 128:]
        for tap in range(2):
            moved = pltpu.roll(prior, 2 - tap, axis=1)
            conv = conv + jnp.concatenate([cols[2 + tap]] * 8, axis=1) * moved[:, 128:]
        value = outer[...] * conv
        for i in range(2):
            part = slice(i * HEAD, (i + 1) * HEAD)
            wide = jnp.concatenate([cols[5, part]] * 8, axis=1)
            cstage[part, :] = norm_rows(value[part], wide).astype(BF16)

    def queries_arrived(k):
        at = pl.ds(k * CHUNK, CHUNK)
        for slot in range(2):
            drain(qbuf.at[slot, pl.ds(0, QROWS), at], qrecv.at[slot, k])

    def lay_keys(b, slot, lo=0, hi=ROWS):
        block = jnp.concatenate(
            [kvbuf[b, HEAD:, lo:hi], jnp.zeros((128 - QROWS, hi - lo), BF16)], axis=0
        )
        kaug[slot, lo:hi] = block.T

    def fold(qs, b, s, tile, keys):
        at = pl.ds(tile * TILE, TILE)
        old = m_ref[qs, :, at]
        new = jnp.maximum(old, jnp.max(s, axis=0, keepdims=True))
        p = jnp.exp2(s - new).astype(BF16)
        factor = jnp.exp2(old - new)
        acc_ref[qs, :, at] = acc_ref[qs, :, at] * factor + jnp.dot(
            kvbuf[b, 0:HEAD, 0:keys], p, preferred_element_type=F32
        )
        m_ref[qs, :, at] = new

    def scores(slot, qs, tile, keys=ROWS):
        return jnp.dot(
            kaug[slot, 0:keys, :], qbuf[qs, :, pl.ds(tile * TILE, TILE)],
            preferred_element_type=F32,
        )

    def masked(s, keys):
        key = lax.broadcasted_iota(jnp.int32, (TILE, TILE), 0)
        query = lax.broadcasted_iota(jnp.int32, (TILE, TILE), 1)
        last = jnp.where(key <= query, s[keys - TILE :, :], -1e30)
        if keys == TILE:
            return last
        return jnp.concatenate([s[: keys - TILE, :], last], axis=0)

    def diagonal(tile):
        keys = (tile + 1) * TILE
        for slot, b in enumerate((own_a, own_b)):
            lay_keys(b, slot, tile * TILE, keys)
        for slot, b in enumerate((own_a, own_b)):
            fold(slot, b, masked(scores(slot, slot, tile, keys), keys), tile, keys)

    queries_arrived(0)
    queries_arrived(1)
    diagonal(0)
    first_hop(2)
    w_second()

    @pl.when(sp > 0)
    def _():
        drain(halo, hsem.at[1])

    mix_conv()
    to_rows = pl.ds(pl.multiple_of(1024 + tp * 128, 128), 128)
    local(
        cstage.at[:, pl.ds(pl.multiple_of(tp * 128, 128), 128)], cbuf.at[to_rows], crecv.at[tp]
    ).start()
    for step in range(1, 8):
        t = (tp + step) % 8
        remote(
            cstage.at[:, pl.ds(pl.multiple_of(t * 128, 128), 128)], cbuf.at[to_rows],
            csend.at[step], crecv.at[tp], {"sp": sp, "tp": t},
        ).start()

    first_hop(3)
    queries_arrived(2)
    queries_arrived(3)
    diagonal(1)
    second_hop(1)
    w_third()

    def run(item, count, ahead):
        qs, b = item(0)
        lay_keys(b, 0)
        s_ref[0] = scores(0, qs, 0)

        def body(n, carry):
            ahead(n + 1)
            qs, b = item(n)
            qn, bn = item(jnp.minimum(n + 1, count - 1))
            cur = n % 2
            s_ref[1] = scores(cur, qs, 1)
            fold(qs, b, s_ref[0], 0, ROWS)
            lay_keys(bn, 1 - cur)
            s_ref[0] = scores(1 - cur, qn, 0)
            fold(qs, b, s_ref[1], 1, ROWS)
            return carry

        lax.fori_loop(0, count, body, 0)

    def pick(n, ys, earlier):
        zero = c + earlier
        in_first = n < zero
        first = jnp.where((c == 1) & (n == 0), 0, set_a)
        return jnp.where(in_first, 0, 1), jnp.where(in_first, first, n - zero) * 4 + ys

    def pick_near(n, ys, earlier):
        k = n - 1 - 2 * earlier
        shared_q = jnp.where((c == 1) & (k == 0), 0, 1)
        shared_z = jnp.where(c == 0, 1 + k, 0)
        qs = jnp.where(k >= 0, shared_q, jnp.where(n == 1, 0, 1))
        zs = jnp.where(k >= 0, shared_z, jnp.where(n == 2, set_b, set_a))
        return qs, zs * 4 + ys

    def send_heads(slot):
        stage[slot] = norm_rows(acc_ref[slot], gbuf[slot][:, 0:1]).astype(BF16)
        head = x * 4 + z
        dst = cbuf.at[pl.ds(pl.multiple_of(head * HEAD, HEAD), HEAD)]
        zt = jnp.where(slot == 0, set_a, set_b)
        for step in range(8):
            t = (tp + step) % 8
            piece = stage.at[slot, :, pl.ds(pl.multiple_of(t * 128, 128), 128)]
            to = {"sp": zt * 4 + y, "tp": t}
            if step:
                remote(piece, dst, osend.at[slot, step], arecv.at[head], to).start()
                continue

            @pl.when(zt == z)
            def _():
                local(piece, dst, arecv.at[head]).start()

            @pl.when(zt != z)
            def _():
                remote(piece, dst, osend.at[slot, step], arecv.at[head], to).start()

    for slot in range(2):
        drain(gbuf.at[slot], grecv.at[slot])
    shared_arrived(y)
    run(lambda n: pick_near(n, y, 0), 3, lambda n: None)
    second_hop(2)
    second_hop(3)
    w_far()

    from_down = jnp.where(down < y, 1, 0)
    from_up = jnp.where(up < y, 1, 0)
    from_far = jnp.where(far < y, 1, 0)
    at_up = 3 + 2 * from_down
    at_far = at_up + 3 + 2 * from_up
    first_far = c + from_far

    def item(n):
        ys = jnp.where(n < at_up, down, jnp.where(n < at_far, up, far))
        earlier = jnp.where(n < at_up, from_down, jnp.where(n < at_far, from_up, from_far))
        start = jnp.where(n < at_up, 0, jnp.where(n < at_far, at_up, at_far))
        late = pick(n - start, ys, earlier)
        soon = pick_near(n - start, ys, earlier)
        return tuple(jnp.where(n < at_far, a, b) for a, b in zip(soon, late))

    def ahead(n):
        @pl.when(n == 1 + 2 * from_down)
        def _():
            shared_arrived(down)

        @pl.when(n == 2)
        def _():
            last_hop(0)
            last_hop(1)

        @pl.when(n == jnp.minimum(8, at_far + first_far))
        def _():
            w_fourth()

        @pl.when(n == at_up)
        def _():
            last_hop(2)
            last_hop(3)
            shared_arrived(up)

        @pl.when(n == at_far)
        def _():
            shared_arrived(far)

    run(item, at_far + first_far, ahead)
    send_heads(0)
    w_fifth()
    run(lambda n: pick(n + first_far, far, from_far), 3 - c + from_far, lambda n: None)
    send_heads(1)

    w_wait(far_x, 0)
    w_send(10, far_x, 0, sib)
    for xx in range(4):
        w_wait(xx * 2 + 1 - c, 0)
        w_wait(xx * 2 + 1 - c, 1)
    for t in range(8):
        drain(cbuf.at[pl.ds(1024 + t * 128, 128)], crecv.at[t])

    def product(lo, n):
        at = pl.ds(n * TILE, TILE)
        return jnp.dot(
            ct[:, lo : lo + 1024], wbuf[lo : lo + 1024, at], preferred_element_type=F32
        )

    def conv_part(n, carry):
        oacc[:, pl.ds(n * TILE, TILE)] = product(1024, n)
        return carry

    ct[:, 1024:] = cbuf[1024:, :].T
    for n in range(WIDTH // TILE):
        conv_part(n, 0)
    for h in range(16):
        drain(cbuf.at[pl.ds(h * HEAD, HEAD)], arecv.at[h])

    def attn_part(n, carry):
        at = pl.ds(n * TILE, TILE)
        out_ref[:, at] = (oacc[:, at] + product(0, n)).astype(BF16)
        return carry

    ct[:, :1024] = cbuf[:1024, :].T
    for n in range(WIDTH // TILE):
        attn_part(n, 0)

    def sent(n, carry):
        for k in range(2):
            drain(rows(tp, n), xsend.at[k, n])
            drain(rows(tp, n, 0), xsend.at[2 + k, n])
        for k in range(4):
            drain(rows(tp, n), xdsend.at[k, n])
        for i in range(2):
            zt = 2 * c + i
            own = (zt == z) & (zc == c)
            at = pl.ds(pl.multiple_of(n * CHUNK, CHUNK), CHUNK)

            @pl.when(jnp.logical_not(own))
            def _():
                drain(kvout.at[i, :, at], zsend.at[i, 0, n])
                drain(qout.at[i, :, at], zsend.at[i, 1, n])

        for k in range(6):
            drain(chunk(0, n), ysend.at[k, n])
        for k in range(4):
            drain(chunk(0, n), dsend.at[k, n])

        @pl.when(c == 1)
        def _():
            for k in range(4, 8):
                drain(chunk(0, n), dsend.at[k, n])

        return carry

    lax.fori_loop(0, 4, sent, 0)
    for i in range(2):
        zt = 2 * c + i
        own = (zt == z) & (zc == c)

        @pl.when(jnp.logical_not(own))
        def _():
            drain(gout.at[i], gsend.at[i])

    @pl.when(sp < 15)
    def _():
        drain(halo, hsem.at[0])

    for n in range(11):
        drain(wbuf.at[pl.ds(0, 128)], wsend.at[n])
    for n in range(6):
        drain(wbuf.at[pl.ds(0, 64)], hsend.at[n])
    for step in range(1, 8):
        drain(cbuf.at[pl.ds(0, 128)], csend.at[step])
    for slot in range(2):
        zt = jnp.where(slot == 0, set_a, set_b)
        piece = stage.at[slot, :, pl.ds(0, 128)]
        for step in range(1, 8):
            drain(piece, osend.at[slot, step])

        @pl.when(zt != z)
        def _():
            drain(piece, osend.at[slot, 0])


def store_kernel(rows, out, sem):
    copy = pltpu.make_async_copy(rows, out, sem)
    copy.start()
    copy.wait()


def per_device(
    tokens, mix_gain, query_weight, key_weight, value_weight, outer_gate_weight,
    inner_gate_weight, conv_input_weight, query_gain, key_gain, gate_totals, conv_taps,
    attn_out_gain, conv_out_gain, attn_out_weight, conv_out_weight,
):
    DMA = pltpu.SemaphoreType.DMA
    far = pl.BlockSpec(memory_space=pl.ANY)
    near = pl.BlockSpec(memory_space=VMEM)
    rows = pl.pallas_call(
        layer_kernel,
        out_shape=pltpu.VMEM((128, WIDTH), BF16),
        in_specs=[far, near] + [far] * 6 + [near] * 6 + [far] * 2,
        out_specs=near,
        scratch_shapes=[
            VMEM((8, ROWS, FEATURES), BF16),
            VMEM((6, WIDTH, 128), BF16),
            VMEM((768, WIDTH), BF16),
            VMEM((CHUNK, WIDTH), BF16),
            VMEM((1, CHUNK), F32),
            VMEM((768, CHUNK), F32),
            VMEM((128, ROWS), F32),
            VMEM((128, ROWS), BF16),
            VMEM((128, 128), BF16),
            VMEM((2, QROWS, ROWS), BF16),
            VMEM((2, KVROWS, ROWS), BF16),
            VMEM((2, HEAD, 128), F32),
            VMEM((6, 128, 128), F32),
            VMEM((2, 128, ROWS), BF16),
            VMEM((16, KVROWS, ROWS), BF16),
            VMEM((2, HEAD, 128), F32),
            VMEM((2, ROWS, 128), BF16),
            VMEM((2, ROWS, TILE), F32),
            VMEM((2, 1, ROWS), F32),
            VMEM((2, HEAD, ROWS), F32),
            VMEM((2, HEAD, ROWS), BF16),
            VMEM((128, ROWS), BF16),
            VMEM((WIDTH, WIDTH), BF16),
            VMEM((WIDTH, 128), BF16),
            VMEM((128, WIDTH), BF16),
            VMEM((128, WIDTH), F32),
            DMA((9,)), DMA((4, 4)), DMA((4, 4)), DMA((8, 4)), DMA((2,)),
            DMA((2, 2, 4)), DMA((2,)), DMA((6, 4)), DMA((8, 4)), DMA((2, 8)), DMA((8,)), DMA((11,)), DMA((6,)),
            DMA((2, 4)), DMA((16, 4)), DMA((2,)), DMA((16,)), DMA((8, 2)), DMA((16,)), DMA((8,)),
        ],
        compiler_params=pltpu.CompilerParams(
            collective_id=1, has_side_effects=True, vmem_limit_bytes=56 * 2**20
        ),
        name="layer",
    )(
        tokens, mix_gain.reshape(1, WIDTH), query_weight, key_weight, value_weight,
        outer_gate_weight, inner_gate_weight, conv_input_weight, query_gain.reshape(1, HEAD),
        key_gain.reshape(1, HEAD), gate_totals.T, conv_taps, attn_out_gain.reshape(1, 128),
        conv_out_gain.reshape(1, 128), attn_out_weight, conv_out_weight,
    )
    return pl.pallas_call(
        store_kernel,
        out_shape=jax.ShapeDtypeStruct((128, WIDTH), BF16),
        in_specs=[near],
        out_specs=far,
        scratch_shapes=[DMA],
        name="store",
    )(pltpu.with_memory_space_constraint(rows, pltpu.VMEM))


def solution(mesh):
    placed = (
        P("sp", "tp"), P(), P(None, "tp"), P(None, "tp"), P(None, "tp"), P(None, "tp"),
        P(None, "tp"), P(None, "tp"), P(), P(), P("sp", "tp"), P(None, "tp"), P("tp"),
        P("tp"), P("tp", None), P("tp", None),
    )
    return jax.shard_map(
        per_device, mesh=mesh, in_specs=placed, out_specs=P(("sp", "tp"), None), check_vma=False
    )
```

```python
import math

import jax
import jax.numpy as jnp
from jax import lax
from jax.experimental import pallas as pl
from jax.experimental.pallas import tpu as pltpu
from jax.sharding import PartitionSpec as P

NORM_EPSILON = 1e-06
MESH = pl.DeviceIdType.MESH
VMEM = pltpu.VMEM
LOG2E = math.log2(math.e)
WIDTH = 2048
ROWS = 1024
CHUNK = 256
FEATURES = 256
HEAD = 64
QROWS = 80
KVROWS = 144
TILE = 512
F32 = jnp.float32
BF16 = jnp.bfloat16


def column(row):
    return jnp.broadcast_to(row, (128, 128)).T


def norm_rows(values, gain):
    scale = lax.rsqrt(jnp.mean(values * values, axis=0, keepdims=True) + NORM_EPSILON)
    return values * scale * gain


def layer_kernel(
    tokens, mix_in, wq, wk, wv, wo, wi, wx, qgain_in, kgain_in, gates_in, taps_in, again_in,
    cgain_in, wa, wc, out_ref, mix, qgain, kgain, gates, taps, again, cgain,
    xbuf, wtmp, wt, xs, scale_ref, proj, outer, gated, halo, qout, kvout, gout, cols,
    qbuf, kvbuf, gbuf, kaug, s_ref, m_ref, acc_ref, stage, cstage, wbuf, cbuf, ct, oacc,
    lsem, xsend, xdsend, xrecv, hsem, zsend, gsend, ysend, dsend, osend, csend, wsend, hsend,
    qrecv, kvrecv, grecv, wrecv, hrecv, arecv, crecv,
):
    sp = lax.axis_index("sp")
    tp = lax.axis_index("tp")
    z, y = sp // 4, sp % 4
    x, c = tp // 2, tp % 2
    zc = jnp.where((z == 1) | (z == 2), 1, 0)
    set_a = c
    set_b = 3 - c

    def dev(zz, yy, xx, cc):
        return {"sp": zz * 4 + yy, "tp": xx * 2 + cc}

    def local(src, dst, sem):
        return pltpu.make_async_copy(src, dst, sem)

    def remote(src, dst, send, recv, to):
        return pltpu.make_async_remote_copy(
            src_ref=src, dst_ref=dst, send_sem=send, recv_sem=recv, device_id=to,
            device_id_type=MESH,
        )

    def drain(ref, sem):
        pltpu.make_async_copy(ref, ref, sem).wait()

    mine = local(tokens, xbuf.at[tp], lsem.at[0])
    mine.start()
    weights = [
        local(w, wtmp.at[n], lsem.at[1 + n]) for n, w in enumerate((wq, wk, wv, wo, wi, wx))
    ]
    own_wa = pl.ds(pl.multiple_of(tp * 128, 128), 128)
    own_wc = pl.ds(pl.multiple_of(1024 + tp * 128, 128), 128)
    out_a = local(wa, wbuf.at[own_wa], lsem.at[7])
    out_c = local(wc, wbuf.at[own_wc], lsem.at[8])
    smalls = [
        local(src, dst, lsem.at[9 + n])
        for n, (src, dst) in enumerate((
            (qgain_in, qgain), (kgain_in, kgain), (gates_in, gates), (taps_in, taps),
            (again_in, again), (cgain_in, cgain), (mix_in, mix),
        ))
    ]
    for small in smalls:
        small.start()

    for w in weights:
        w.start()
    out_a.start()
    out_c.start()
    barrier = pltpu.get_barrier_semaphore()

    def greet(step, carry):
        other = (z * 8 + tp + step) % 32
        pl.semaphore_signal(
            barrier, inc=1, device_id={"sp": (other // 8) * 4 + y, "tp": other % 8},
            device_id_type=MESH,
        )
        return carry

    lax.fori_loop(1, 32, greet, 0)
    for step in (1, 3):
        pl.semaphore_signal(
            barrier, inc=1, device_id=dev(z, (y + step) % 4, x, c), device_id_type=MESH
        )
    for step in (1, 15):
        pl.semaphore_signal(
            barrier, inc=1, device_id={"sp": (sp + step) % 16, "tp": tp}, device_id_type=MESH
        )
    mine.wait()
    pl.semaphore_wait(barrier, 35)

    right, left, across_x = (x + 1) % 4, (x + 3) % 4, (x + 2) % 4
    sib = dev(z, y, x, 1 - c)

    def rows(t, n, half=None):
        if half is None:
            return xbuf.at[t, pl.ds(pl.multiple_of(n * CHUNK, CHUNK), CHUNK)]
        return xbuf.at[t, pl.ds(pl.multiple_of(n * CHUNK + half * 128, 128), 128)]

    def send_own(n):
        piece = rows(tp, n)
        remote(piece, piece, xsend.at[0, n], xrecv.at[tp, n], dev(z, y, right, c)).start()
        remote(piece, piece, xsend.at[1, n], xrecv.at[tp, n], dev(z, y, left, c)).start()
        remote(piece, piece, xdsend.at[0, n], xrecv.at[tp, n], sib).start()

    send_own(0)
    send_own(1)

    for small in smalls:
        small.wait()
    for n, row in enumerate((qgain, kgain)):
        both = jnp.concatenate([row[...], row[...]], axis=1)
        if n == 0:
            both = both * (LOG2E * HEAD**-0.5)
        cols[n] = column(both)
    for n in range(3):
        cols[2 + n] = column(taps[n : n + 1, :])
    cols[5] = column(cgain[...])
    out_gain = column(again[...])
    for i in range(2):
        gout[i] = out_gain[i * HEAD : (i + 1) * HEAD]
    spot = lax.broadcasted_iota(jnp.int32, (16, ROWS), 0)
    for i in range(2):
        g = gates[i : i + 1, :] * LOG2E
        hi = g.astype(BF16).astype(F32)
        mid = (g - hi).astype(BF16).astype(F32)
        low = g - hi - mid
        one = jnp.where(spot < 3, 1.0, 0.0)
        parts = jnp.where(spot == 3, hi, jnp.where(spot == 4, mid, jnp.where(spot == 5, low, one)))
        qout[i, HEAD:, :] = parts.astype(BF16)
        one = jnp.where((spot > 2) & (spot < 6), 1.0, 0.0)
        parts = jnp.where(spot == 0, -hi, jnp.where(spot == 1, -mid, jnp.where(spot == 2, -low, one)))
        kvout[i, 2 * HEAD :, :] = parts.astype(BF16)
    for n, w in enumerate(weights):
        w.wait()
        for k in range(4):
            wt[n * 128 : (n + 1) * 128, k * 512 : (k + 1) * 512] = wtmp[
                n, k * 512 : (k + 1) * 512, :
            ].T

    for slot in range(2):
        qbuf[slot, QROWS:, :] = jnp.zeros((128 - QROWS, ROWS), BF16)
    m_ref[...] = jnp.full_like(m_ref, -1e30)
    acc_ref[...] = jnp.zeros_like(acc_ref)

    @pl.when(sp == 0)
    def _():
        halo[...] = jnp.zeros_like(halo)

    qslot = z // 2

    def z_sends(n):
        at = pl.ds(pl.multiple_of(n * CHUNK, CHUNK), CHUNK)
        for i in range(2):
            zt = 2 * c + i
            own = (zt == z) & (zc == c)
            pieces = (
                (kvout.at[i, :, at], kvbuf.at[sp, :, at], kvrecv.at[sp, n]),
                (qout.at[i, :, at], qbuf.at[qslot, pl.ds(0, QROWS), at], qrecv.at[qslot, n]),
            )

            @pl.when(own)
            def _():
                for src, dst, recv in pieces:
                    local(src, dst, recv).start()

            @pl.when(jnp.logical_not(own))
            def _():
                for k, (src, dst, recv) in enumerate(pieces):
                    remote(src, dst, zsend.at[i, k, n], recv, dev(zt, y, x, zc)).start()

    for i in range(2):
        zt = 2 * c + i
        own = (zt == z) & (zc == c)

        @pl.when(own)
        def _():
            local(gout.at[i], gbuf.at[qslot], grecv.at[qslot]).start()

        @pl.when(jnp.logical_not(own))
        def _():
            remote(
                gout.at[i], gbuf.at[qslot], gsend.at[i], grecv.at[qslot], dev(zt, y, x, zc)
            ).start()

    def project(n):
        at = pl.ds(pl.multiple_of(n * CHUNK, CHUNK), CHUNK)
        squares = jnp.zeros((CHUNK, 128), F32)
        for t in range(8):
            piece = xbuf[t, at, :].astype(F32)
            squares = squares + piece[:, :128] * piece[:, :128] + piece[:, 128:] * piece[:, 128:]
            lanes = slice(t * FEATURES, (t + 1) * FEATURES)
            xs[n, :, lanes] = (piece * mix[:, lanes]).astype(BF16)
        total = jnp.sum(squares.T, axis=0, keepdims=True)
        row_scale = lax.rsqrt(total / WIDTH + NORM_EPSILON)
        scale_ref[n] = row_scale
        proj[0:384] = lax.dot_general(
            wt[0:384], xs[n], (((1,), (1,)), ((), ())), preferred_element_type=F32
        ) * row_scale
        for i in range(2):
            lo = i * HEAD
            wide = [
                jnp.concatenate([cols[k, lo : lo + HEAD]] * 2, axis=1) for k in range(2)
            ]
            qout[i, 0:HEAD, at] = norm_rows(proj[lo : lo + HEAD], wide[0]).astype(BF16)
            kvout[i, HEAD : 2 * HEAD, at] = norm_rows(
                proj[128 + lo : 128 + lo + HEAD], wide[1]
            ).astype(BF16)
            kvout[i, 0:HEAD, at] = proj[256 + lo : 256 + lo + HEAD].astype(BF16)

    def project_conv(n):
        at = pl.ds(pl.multiple_of(n * CHUNK, CHUNK), CHUNK)
        proj[384:768] = lax.dot_general(
            wt[384:768], xs[n], (((1,), (1,)), ((), ())), preferred_element_type=F32
        ) * scale_ref[n]
        outer[:, at] = proj[384:512]
        gated[:, at] = (proj[512:640] * proj[640:768]).astype(BF16)

    def chunk(b, k):
        return kvbuf.at[b, :, pl.ds(pl.multiple_of(k * CHUNK, CHUNK), CHUNK)]

    def arrived(b, k):
        drain(chunk(b, k), kvrecv.at[b, k])

    def along(n, b, k, yy):
        piece = chunk(b, k)
        remote(piece, piece, ysend.at[n, k], kvrecv.at[b, k], dev(z, yy, x, c)).start()

    def across(n, b, k):
        piece = chunk(b, k)
        remote(piece, piece, dsend.at[n, k], kvrecv.at[b, k], sib).start()

    up, down, far = (y + 1) % 4, (y + 3) % 4, (y + 2) % 4
    own_a, own_b = set_a * 4 + y, set_b * 4 + y

    def share_a(n, ys, k):
        across(n, set_a * 4 + ys, k)

    def share_b(n, ys, k):
        @pl.when(c == 1)
        def _():
            across(4 + n, set_b * 4 + ys, k)

    def first_hop(k):
        arrived(own_a, k)
        along(0, own_a, k, up)
        arrived(own_b, k)
        along(1, own_b, k, down)
        along(2, own_b, k, up)
        along(3, own_a, k, down)
        share_a(0, y, k)
        share_b(0, y, k)

    def second_hop(k):
        arrived(set_a * 4 + down, k)
        along(4, set_a * 4 + down, k, up)
        arrived(set_b * 4 + up, k)
        along(5, set_b * 4 + up, k, down)
        share_a(1, down, k)
        share_b(2, up, k)
        arrived(set_b * 4 + down, k)
        share_b(1, down, k)
        arrived(set_a * 4 + up, k)
        share_a(2, up, k)

    def last_hop(k):
        arrived(set_a * 4 + far, k)
        share_a(3, far, k)
        arrived(set_b * 4 + far, k)
        share_b(3, far, k)

    def shared_arrived(ys):
        @pl.when(c == 0)
        def _():
            for k in range(4):
                arrived(4 + ys, k)
                arrived(8 + ys, k)

        @pl.when(c == 1)
        def _():
            for k in range(4):
                arrived(ys, k)

    def w_rows(t, kind):
        return pl.ds(pl.multiple_of(kind * 1024 + t * 128, 128), 128)

    def w_send(n, t, kind, to):
        piece = wbuf.at[w_rows(t, kind)]
        remote(piece, piece, wsend.at[n], wrecv.at[kind * 8 + t], to).start()

    def w_wait(t, kind):
        drain(wbuf.at[w_rows(t, kind)], wrecv.at[kind * 8 + t])

    before, after, far_x = left * 2 + c, right * 2 + c, across_x * 2 + c
    near_z = z + 1 - 2 * (z % 2)

    def h_rows(t, half):
        return wbuf.at[pl.ds(pl.multiple_of(1024 + t * 128 + half * 64, 64), 64)]

    def h_send(n, t, to):
        piece = h_rows(t, z % 2)
        remote(piece, piece, hsend.at[n], hrecv.at[t, z % 2], to).start()

    def h_wait(t, half):
        drain(h_rows(t, half), hrecv.at[t, half])

    def w_first():
        out_a.wait()
        out_c.wait()
        h_send(0, tp, dev(z, y, right, c))
        h_send(1, tp, dev(z, y, left, c))
        w_send(2, tp, 0, sib)
        w_send(3, tp, 1, sib)

    def w_second():
        h_wait(before, z % 2)
        h_wait(after, z % 2)

        @pl.when(c == 0)
        def _():
            h_send(2, before, dev(z, y, right, c))

        @pl.when(c == 1)
        def _():
            h_send(2, after, dev(z, y, left, c))

        w_send(0, tp, 0, dev(z, y, right, c))
        w_send(1, tp, 0, dev(z, y, left, c))

    def w_third():
        partner = dev(near_z, y, x, c)
        h_send(3, before, partner)
        h_send(4, after, partner)

    def w_far():
        h_wait(far_x, z % 2)
        h_send(5, far_x, dev(near_z, y, x, c))

    def w_fourth():
        w_wait(before, 0)
        w_wait(after, 0)

        @pl.when(c == 0)
        def _():
            w_send(4, before, 0, dev(z, y, right, c))

        @pl.when(c == 1)
        def _():
            w_send(4, after, 0, dev(z, y, left, c))

        w_send(5, before, 0, sib)
        w_send(6, after, 0, sib)

    def w_fifth():
        for n, t in enumerate((before, after, far_x)):
            h_wait(t, 1 - z % 2)
            w_send(7 + n, t, 1, sib)

    def gather(n, carry):
        @pl.when(n < 4)
        def _():
            drain(rows(before, n), xrecv.at[before, n])
            piece = rows(before, n, 0)
            remote(piece, piece, xsend.at[2, n], xrecv.at[before, n], dev(z, y, right, c)).start()
            piece = rows(before, n)
            remote(piece, piece, xdsend.at[1, n], xrecv.at[before, n], sib).start()
            drain(rows(after, n), xrecv.at[after, n])
            piece = rows(after, n, 1)
            remote(piece, piece, xsend.at[3, n], xrecv.at[after, n], dev(z, y, left, c)).start()
            piece = rows(after, n)
            remote(piece, piece, xdsend.at[2, n], xrecv.at[after, n], sib).start()

            @pl.when(n < 2)
            def _():
                send_own(n + 2)

            @pl.when(n == 3)
            def _():
                w_first()

        @pl.when(n > 0)
        def _():
            done = n - 1
            far = across_x * 2 + c
            drain(rows(far, done), xrecv.at[far, done])
            piece = rows(far, done)
            remote(piece, piece, xdsend.at[3, done], xrecv.at[far, done], sib).start()
            for xx in range(4):
                t = xx * 2 + 1 - c
                drain(rows(t, done), xrecv.at[t, done])
            project(done)
            z_sends(done)

        @pl.when((n > 1) & (n < 4))
        def _():
            first_hop(n - 2)

        @pl.when(n == 3)
        def _():
            second_hop(n - 3)

        return carry

    lax.fori_loop(0, 5, gather, 0)
    project_conv(3)

    @pl.when(sp < 15)
    def _():
        remote(
            gated.at[:, pl.ds(ROWS - 128, 128)], halo, hsem.at[0], hsem.at[1],
            {"sp": jnp.minimum(sp + 1, 15), "tp": tp},
        ).start()

    def mix_conv():
        prior = jnp.concatenate([halo[...], gated[...]], axis=1).astype(F32)
        conv = jnp.concatenate([cols[4]] * 8, axis=1) * prior[:, 128:]
        for tap in range(2):
            moved = pltpu.roll(prior, 2 - tap, axis=1)
            conv = conv + jnp.concatenate([cols[2 + tap]] * 8, axis=1) * moved[:, 128:]
        value = outer[...] * conv
        for i in range(2):
            part = slice(i * HEAD, (i + 1) * HEAD)
            wide = jnp.concatenate([cols[5, part]] * 8, axis=1)
            cstage[part, :] = norm_rows(value[part], wide).astype(BF16)

    def queries_arrived(k):
        at = pl.ds(k * CHUNK, CHUNK)
        for slot in range(2):
            drain(qbuf.at[slot, pl.ds(0, QROWS), at], qrecv.at[slot, k])

    def lay_keys(b, slot, lo=0, hi=ROWS):
        block = jnp.concatenate(
            [kvbuf[b, HEAD:, lo:hi], jnp.zeros((128 - QROWS, hi - lo), BF16)], axis=0
        )
        kaug[slot, lo:hi] = block.T

    def fold(qs, b, s, tile, keys):
        at = pl.ds(tile * TILE, TILE)
        old = m_ref[qs, :, at]
        new = jnp.maximum(old, jnp.max(s, axis=0, keepdims=True))
        p = jnp.exp2(s - new).astype(BF16)
        factor = jnp.exp2(old - new)
        acc_ref[qs, :, at] = acc_ref[qs, :, at] * factor + jnp.dot(
            kvbuf[b, 0:HEAD, 0:keys], p, preferred_element_type=F32
        )
        m_ref[qs, :, at] = new

    def scores(slot, qs, tile, keys=ROWS):
        return jnp.dot(
            kaug[slot, 0:keys, :], qbuf[qs, :, pl.ds(tile * TILE, TILE)],
            preferred_element_type=F32,
        )

    def masked(s, keys):
        key = lax.broadcasted_iota(jnp.int32, (TILE, TILE), 0)
        query = lax.broadcasted_iota(jnp.int32, (TILE, TILE), 1)
        last = jnp.where(key <= query, s[keys - TILE :, :], -1e30)
        if keys == TILE:
            return last
        return jnp.concatenate([s[: keys - TILE, :], last], axis=0)

    def diagonal(tile):
        keys = (tile + 1) * TILE
        for slot, b in enumerate((own_a, own_b)):
            lay_keys(b, slot, tile * TILE, keys)
        for slot, b in enumerate((own_a, own_b)):
            fold(slot, b, masked(scores(slot, slot, tile, keys), keys), tile, keys)

    queries_arrived(0)
    queries_arrived(1)
    diagonal(0)
    first_hop(2)
    w_second()

    def conv_rest(n, carry):
        project_conv(n)
        return carry

    lax.fori_loop(0, 3, conv_rest, 0)
    first_hop(3)
    queries_arrived(2)
    queries_arrived(3)
    diagonal(1)
    second_hop(1)
    w_third()

    @pl.when(sp > 0)
    def _():
        drain(halo, hsem.at[1])

    mix_conv()
    to_rows = pl.ds(pl.multiple_of(1024 + tp * 128, 128), 128)
    local(
        cstage.at[:, pl.ds(pl.multiple_of(tp * 128, 128), 128)], cbuf.at[to_rows], crecv.at[tp]
    ).start()
    for step in range(1, 8):
        t = (tp + step) % 8
        remote(
            cstage.at[:, pl.ds(pl.multiple_of(t * 128, 128), 128)], cbuf.at[to_rows],
            csend.at[step], crecv.at[tp], {"sp": sp, "tp": t},
        ).start()


    def run(item, count, ahead):
        qs, b = item(0)
        lay_keys(b, 0)
        s_ref[0] = scores(0, qs, 0)

        def body(n, carry):
            ahead(n + 1)
            qs, b = item(n)
            qn, bn = item(jnp.minimum(n + 1, count - 1))
            cur = n % 2
            s_ref[1] = scores(cur, qs, 1)
            fold(qs, b, s_ref[0], 0, ROWS)
            lay_keys(bn, 1 - cur)
            s_ref[0] = scores(1 - cur, qn, 0)
            fold(qs, b, s_ref[1], 1, ROWS)
            return carry

        lax.fori_loop(0, count, body, 0)

    def pick(n, ys, earlier):
        zero = c + earlier
        in_first = n < zero
        first = jnp.where((c == 1) & (n == 0), 0, set_a)
        return jnp.where(in_first, 0, 1), jnp.where(in_first, first, n - zero) * 4 + ys

    def pick_near(n, ys, earlier):
        k = n - 1 - 2 * earlier
        shared_q = jnp.where((c == 1) & (k == 0), 0, 1)
        shared_z = jnp.where(c == 0, 1 + k, 0)
        qs = jnp.where(k >= 0, shared_q, jnp.where(n == 1, 0, 1))
        zs = jnp.where(k >= 0, shared_z, jnp.where(n == 2, set_b, set_a))
        return qs, zs * 4 + ys

    def send_heads(slot):
        stage[slot] = norm_rows(acc_ref[slot], gbuf[slot][:, 0:1]).astype(BF16)
        head = x * 4 + z
        dst = cbuf.at[pl.ds(pl.multiple_of(head * HEAD, HEAD), HEAD)]
        zt = jnp.where(slot == 0, set_a, set_b)
        for step in range(8):
            t = (tp + step) % 8
            piece = stage.at[slot, :, pl.ds(pl.multiple_of(t * 128, 128), 128)]
            to = {"sp": zt * 4 + y, "tp": t}
            if step:
                remote(piece, dst, osend.at[slot, step], arecv.at[head], to).start()
                continue

            @pl.when(zt == z)
            def _():
                local(piece, dst, arecv.at[head]).start()

            @pl.when(zt != z)
            def _():
                remote(piece, dst, osend.at[slot, step], arecv.at[head], to).start()

    for slot in range(2):
        drain(gbuf.at[slot], grecv.at[slot])
    shared_arrived(y)
    run(lambda n: pick_near(n, y, 0), 3, lambda n: None)
    second_hop(2)
    second_hop(3)
    w_far()

    from_down = jnp.where(down < y, 1, 0)
    from_up = jnp.where(up < y, 1, 0)
    from_far = jnp.where(far < y, 1, 0)
    at_up = 3 + 2 * from_down
    at_far = at_up + 3 + 2 * from_up
    first_far = c + from_far

    def item(n):
        ys = jnp.where(n < at_up, down, jnp.where(n < at_far, up, far))
        earlier = jnp.where(n < at_up, from_down, jnp.where(n < at_far, from_up, from_far))
        start = jnp.where(n < at_up, 0, jnp.where(n < at_far, at_up, at_far))
        late = pick(n - start, ys, earlier)
        soon = pick_near(n - start, ys, earlier)
        return tuple(jnp.where(n < at_far, a, b) for a, b in zip(soon, late))

    def ahead(n):
        @pl.when(n == 1 + 2 * from_down)
        def _():
            shared_arrived(down)

        @pl.when(n == 2)
        def _():
            last_hop(0)
            last_hop(1)

        @pl.when(n == jnp.minimum(8, at_far + first_far))
        def _():
            w_fourth()

        @pl.when(n == at_up)
        def _():
            last_hop(2)
            last_hop(3)
            shared_arrived(up)

        @pl.when(n == at_far)
        def _():
            shared_arrived(far)

    run(item, at_far + first_far, ahead)
    send_heads(0)
    run(lambda n: pick(n + first_far, far, from_far), 3 - c + from_far, lambda n: None)
    send_heads(1)
    w_fifth()

    w_wait(far_x, 0)
    w_send(10, far_x, 0, sib)
    for xx in range(4):
        w_wait(xx * 2 + 1 - c, 0)
        w_wait(xx * 2 + 1 - c, 1)
    for t in range(8):
        drain(cbuf.at[pl.ds(1024 + t * 128, 128)], crecv.at[t])

    def product(lo, n):
        at = pl.ds(n * TILE, TILE)
        return jnp.dot(
            ct[:, lo : lo + 1024], wbuf[lo : lo + 1024, at], preferred_element_type=F32
        )

    def conv_part(n, carry):
        oacc[:, pl.ds(n * TILE, TILE)] = product(1024, n)
        return carry

    ct[:, 1024:] = cbuf[1024:, :].T
    for n in range(WIDTH // TILE):
        conv_part(n, 0)
    for h in range(16):
        drain(cbuf.at[pl.ds(h * HEAD, HEAD)], arecv.at[h])

    def attn_part(n, carry):
        at = pl.ds(n * TILE, TILE)
        out_ref[:, at] = (oacc[:, at] + product(0, n)).astype(BF16)
        return carry

    ct[:, :1024] = cbuf[:1024, :].T
    for n in range(WIDTH // TILE):
        attn_part(n, 0)

    def sent(n, carry):
        for k in range(2):
            drain(rows(tp, n), xsend.at[k, n])
            drain(rows(tp, n, 0), xsend.at[2 + k, n])
        for k in range(4):
            drain(rows(tp, n), xdsend.at[k, n])
        for i in range(2):
            zt = 2 * c + i
            own = (zt == z) & (zc == c)
            at = pl.ds(pl.multiple_of(n * CHUNK, CHUNK), CHUNK)

            @pl.when(jnp.logical_not(own))
            def _():
                drain(kvout.at[i, :, at], zsend.at[i, 0, n])
                drain(qout.at[i, :, at], zsend.at[i, 1, n])

        for k in range(6):
            drain(chunk(0, n), ysend.at[k, n])
        for k in range(4):
            drain(chunk(0, n), dsend.at[k, n])

        @pl.when(c == 1)
        def _():
            for k in range(4, 8):
                drain(chunk(0, n), dsend.at[k, n])

        return carry

    lax.fori_loop(0, 4, sent, 0)
    for i in range(2):
        zt = 2 * c + i
        own = (zt == z) & (zc == c)

        @pl.when(jnp.logical_not(own))
        def _():
            drain(gout.at[i], gsend.at[i])

    @pl.when(sp < 15)
    def _():
        drain(halo, hsem.at[0])

    for n in range(11):
        drain(wbuf.at[pl.ds(0, 128)], wsend.at[n])
    for n in range(6):
        drain(wbuf.at[pl.ds(0, 64)], hsend.at[n])
    for step in range(1, 8):
        drain(cbuf.at[pl.ds(0, 128)], csend.at[step])
    for slot in range(2):
        zt = jnp.where(slot == 0, set_a, set_b)
        piece = stage.at[slot, :, pl.ds(0, 128)]
        for step in range(1, 8):
            drain(piece, osend.at[slot, step])

        @pl.when(zt != z)
        def _():
            drain(piece, osend.at[slot, 0])


def store_kernel(rows, out, sem):
    copy = pltpu.make_async_copy(rows, out, sem)
    copy.start()
    copy.wait()


def per_device(
    tokens, mix_gain, query_weight, key_weight, value_weight, outer_gate_weight,
    inner_gate_weight, conv_input_weight, query_gain, key_gain, gate_totals, conv_taps,
    attn_out_gain, conv_out_gain, attn_out_weight, conv_out_weight,
):
    DMA = pltpu.SemaphoreType.DMA
    far = pl.BlockSpec(memory_space=pl.ANY)
    near = pl.BlockSpec(memory_space=VMEM)
    rows = pl.pallas_call(
        layer_kernel,
        out_shape=pltpu.VMEM((128, WIDTH), BF16),
        in_specs=[far] * 16,
        out_specs=near,
        scratch_shapes=[
            VMEM((1, WIDTH), F32),
            VMEM((1, HEAD), F32),
            VMEM((1, HEAD), F32),
            VMEM((2, ROWS), F32),
            VMEM((3, 128), F32),
            VMEM((1, 128), F32),
            VMEM((1, 128), F32),
            VMEM((8, ROWS, FEATURES), BF16),
            VMEM((6, WIDTH, 128), BF16),
            VMEM((768, WIDTH), BF16),
            VMEM((4, CHUNK, WIDTH), BF16),
            VMEM((4, 1, CHUNK), F32),
            VMEM((768, CHUNK), F32),
            VMEM((128, ROWS), F32),
            VMEM((128, ROWS), BF16),
            VMEM((128, 128), BF16),
            VMEM((2, QROWS, ROWS), BF16),
            VMEM((2, KVROWS, ROWS), BF16),
            VMEM((2, HEAD, 128), F32),
            VMEM((6, 128, 128), F32),
            VMEM((2, 128, ROWS), BF16),
            VMEM((16, KVROWS, ROWS), BF16),
            VMEM((2, HEAD, 128), F32),
            VMEM((2, ROWS, 128), BF16),
            VMEM((2, ROWS, TILE), F32),
            VMEM((2, 1, ROWS), F32),
            VMEM((2, HEAD, ROWS), F32),
            VMEM((2, HEAD, ROWS), BF16),
            VMEM((128, ROWS), BF16),
            VMEM((WIDTH, WIDTH), BF16),
            VMEM((WIDTH, 128), BF16),
            VMEM((128, WIDTH), BF16),
            VMEM((128, WIDTH), F32),
            DMA((16,)), DMA((4, 4)), DMA((4, 4)), DMA((8, 4)), DMA((2,)),
            DMA((2, 2, 4)), DMA((2,)), DMA((6, 4)), DMA((8, 4)), DMA((2, 8)), DMA((8,)), DMA((11,)), DMA((6,)),
            DMA((2, 4)), DMA((16, 4)), DMA((2,)), DMA((16,)), DMA((8, 2)), DMA((16,)), DMA((8,)),
        ],
        compiler_params=pltpu.CompilerParams(
            collective_id=1, has_side_effects=True, vmem_limit_bytes=56 * 2**20
        ),
        name="layer",
    )(
        tokens, mix_gain.reshape(1, WIDTH), query_weight, key_weight, value_weight,
        outer_gate_weight, inner_gate_weight, conv_input_weight, query_gain.reshape(1, HEAD),
        key_gain.reshape(1, HEAD), gate_totals.T, conv_taps, attn_out_gain.reshape(1, 128),
        conv_out_gain.reshape(1, 128), attn_out_weight, conv_out_weight,
    )
    return pl.pallas_call(
        store_kernel,
        out_shape=jax.ShapeDtypeStruct((128, WIDTH), BF16),
        in_specs=[near],
        out_specs=far,
        scratch_shapes=[DMA],
        name="store",
    )(pltpu.with_memory_space_constraint(rows, pltpu.VMEM))


def solution(mesh):
    placed = (
        P("sp", "tp"), P(), P(None, "tp"), P(None, "tp"), P(None, "tp"), P(None, "tp"),
        P(None, "tp"), P(None, "tp"), P(), P(), P("sp", "tp"), P(None, "tp"), P("tp"),
        P("tp"), P("tp", None), P("tp", None),
    )
    return jax.shard_map(
        per_device, mesh=mesh, in_specs=placed, out_specs=P(("sp", "tp"), None), check_vma=False
    )
```

```python
import math

import jax
import jax.numpy as jnp
from jax import lax
from jax.experimental import pallas as pl
from jax.experimental.pallas import tpu as pltpu
from jax.sharding import PartitionSpec as P

NORM_EPSILON = 1e-06
MESH = pl.DeviceIdType.MESH
VMEM = pltpu.VMEM
LOG2E = math.log2(math.e)
WIDTH = 2048
ROWS = 1024
CHUNK = 256
FEATURES = 256
HEAD = 64
QROWS = 80
KVROWS = 144
TILE = 512
F32 = jnp.float32
BF16 = jnp.bfloat16


def column(row):
    return jnp.broadcast_to(row, (128, 128)).T


def norm_rows(values, gain):
    scale = lax.rsqrt(jnp.mean(values * values, axis=0, keepdims=True) + NORM_EPSILON)
    return values * scale * gain


def layer_kernel(
    tokens, mix_in, wq, wk, wv, wo, wi, wx, qgain_in, kgain_in, gates_in, taps_in, again_in,
    cgain_in, wa, wc, out_ref, mix, qgain, kgain, gates, taps, again, cgain,
    xbuf, wtmp, wt, xs, scale_ref, proj, outer, gated, halo, qout, kvout, gout, cols,
    qbuf, kvbuf, gbuf, kaug, s_ref, m_ref, acc_ref, stage, cstage, wbuf, cbuf, ct, oacc,
    lsem, xsend, xdsend, xrecv, xshare, hsem, zsend, gsend, ysend, dsend, osend, csend, wsend,
    hsend, hdsend, qrecv, kvrecv, kvshare, grecv, wrecv, wshare, hrecv, hshare, arecv, crecv,
):
    sp = lax.axis_index("sp")
    tp = lax.axis_index("tp")
    z, y = sp // 4, sp % 4
    x, c = tp // 2, tp % 2
    zc = jnp.where((z == 1) | (z == 2), 1, 0)
    set_a = c
    set_b = 3 - c

    def dev(zz, yy, xx, cc):
        return {"sp": zz * 4 + yy, "tp": xx * 2 + cc}

    def local(src, dst, sem):
        return pltpu.make_async_copy(src, dst, sem)

    def remote(src, dst, send, recv, to):
        return pltpu.make_async_remote_copy(
            src_ref=src, dst_ref=dst, send_sem=send, recv_sem=recv, device_id=to,
            device_id_type=MESH,
        )

    def drain(ref, sem):
        pltpu.make_async_copy(ref, ref, sem).wait()

    mine = local(tokens, xbuf.at[tp], lsem.at[0])
    mine.start()
    weights = [
        local(w, wtmp.at[n], lsem.at[1 + n]) for n, w in enumerate((wq, wk, wv, wo, wi, wx))
    ]
    own_wa = pl.ds(pl.multiple_of(tp * 128, 128), 128)
    own_wc = pl.ds(pl.multiple_of(1024 + tp * 128, 128), 128)
    out_a = local(wa, wbuf.at[own_wa], lsem.at[7])
    out_c = local(wc, wbuf.at[own_wc], lsem.at[8])
    smalls = [
        local(src, dst, lsem.at[9 + n])
        for n, (src, dst) in enumerate((
            (qgain_in, qgain), (kgain_in, kgain), (gates_in, gates), (taps_in, taps),
            (again_in, again), (cgain_in, cgain), (mix_in, mix),
        ))
    ]
    for small in smalls:
        small.start()

    for w in weights:
        w.start()
    out_a.start()
    out_c.start()
    barrier = pltpu.get_barrier_semaphore()

    def greet(step, carry):
        other = (z * 8 + tp + step) % 32
        pl.semaphore_signal(
            barrier, inc=1, device_id={"sp": (other // 8) * 4 + y, "tp": other % 8},
            device_id_type=MESH,
        )
        return carry

    lax.fori_loop(1, 32, greet, 0)
    for step in (1, 3):
        pl.semaphore_signal(
            barrier, inc=1, device_id=dev(z, (y + step) % 4, x, c), device_id_type=MESH
        )
    for step in (1, 15):
        pl.semaphore_signal(
            barrier, inc=1, device_id={"sp": (sp + step) % 16, "tp": tp}, device_id_type=MESH
        )
    mine.wait()
    pl.semaphore_wait(barrier, 35)

    right, left, across_x = (x + 1) % 4, (x + 3) % 4, (x + 2) % 4
    sib = dev(z, y, x, 1 - c)

    def rows(t, n, half=None):
        if half is None:
            return xbuf.at[t, pl.ds(pl.multiple_of(n * CHUNK, CHUNK), CHUNK)]
        return xbuf.at[t, pl.ds(pl.multiple_of(n * CHUNK + half * 128, 128), 128)]

    def send_own(n):
        piece = rows(tp, n)
        remote(piece, piece, xsend.at[0], xrecv.at[tp // 2, n], dev(z, y, right, c)).start()
        remote(piece, piece, xsend.at[0], xrecv.at[tp // 2, n], dev(z, y, left, c)).start()
        remote(piece, piece, xdsend.at[0], xshare.at[n], sib).start()

    send_own(0)
    send_own(1)

    for small in smalls:
        small.wait()
    for n, row in enumerate((qgain, kgain)):
        both = jnp.concatenate([row[...], row[...]], axis=1)
        if n == 0:
            both = both * (LOG2E * HEAD**-0.5)
        cols[n] = column(both)
    for n in range(3):
        cols[2 + n] = column(taps[n : n + 1, :])
    cols[5] = column(cgain[...])
    out_gain = column(again[...])
    for i in range(2):
        gout[i] = out_gain[i * HEAD : (i + 1) * HEAD]
    spot = lax.broadcasted_iota(jnp.int32, (16, ROWS), 0)
    for i in range(2):
        g = gates[i : i + 1, :] * LOG2E
        hi = g.astype(BF16).astype(F32)
        mid = (g - hi).astype(BF16).astype(F32)
        low = g - hi - mid
        one = jnp.where(spot < 3, 1.0, 0.0)
        parts = jnp.where(spot == 3, hi, jnp.where(spot == 4, mid, jnp.where(spot == 5, low, one)))
        qout[i, HEAD:, :] = parts.astype(BF16)
        one = jnp.where((spot > 2) & (spot < 6), 1.0, 0.0)
        parts = jnp.where(spot == 0, -hi, jnp.where(spot == 1, -mid, jnp.where(spot == 2, -low, one)))
        kvout[i, 2 * HEAD :, :] = parts.astype(BF16)
    for n, w in enumerate(weights):
        w.wait()
        for k in range(4):
            wt[n * 128 : (n + 1) * 128, k * 512 : (k + 1) * 512] = wtmp[
                n, k * 512 : (k + 1) * 512, :
            ].T

    for slot in range(2):
        qbuf[slot, QROWS:, :] = jnp.zeros((128 - QROWS, ROWS), BF16)
    m_ref[...] = jnp.full_like(m_ref, -1e30)
    acc_ref[...] = jnp.zeros_like(acc_ref)

    @pl.when(sp == 0)
    def _():
        halo[...] = jnp.zeros_like(halo)

    qslot = z // 2

    def native(b):
        return jnp.where(b < 8, 0, 4) + b % 4

    def z_sends(n):
        at = pl.ds(pl.multiple_of(n * CHUNK, CHUNK), CHUNK)
        for i in range(2):
            zt = 2 * c + i
            own = (zt == z) & (zc == c)
            pieces = (
                (kvout.at[i, :, at], kvbuf.at[sp, :, at], kvrecv.at[native(sp), n]),
                (qout.at[i, :, at], qbuf.at[qslot, pl.ds(0, QROWS), at], qrecv.at[qslot, n]),
            )

            @pl.when(own)
            def _():
                for src, dst, recv in pieces:
                    local(src, dst, recv).start()

            @pl.when(jnp.logical_not(own))
            def _():
                for k, (src, dst, recv) in enumerate(pieces):
                    remote(src, dst, zsend.at[i, k], recv, dev(zt, y, x, zc)).start()

    for i in range(2):
        zt = 2 * c + i
        own = (zt == z) & (zc == c)

        @pl.when(own)
        def _():
            local(gout.at[i], gbuf.at[qslot], grecv.at[qslot]).start()

        @pl.when(jnp.logical_not(own))
        def _():
            remote(
                gout.at[i], gbuf.at[qslot], gsend.at[i], grecv.at[qslot], dev(zt, y, x, zc)
            ).start()

    def project(n):
        at = pl.ds(pl.multiple_of(n * CHUNK, CHUNK), CHUNK)
        squares = jnp.zeros((CHUNK, 128), F32)
        for t in range(8):
            piece = xbuf[t, at, :].astype(F32)
            squares = squares + piece[:, :128] * piece[:, :128] + piece[:, 128:] * piece[:, 128:]
            lanes = slice(t * FEATURES, (t + 1) * FEATURES)
            xs[n, :, lanes] = (piece * mix[:, lanes]).astype(BF16)
        total = jnp.sum(squares.T, axis=0, keepdims=True)
        row_scale = lax.rsqrt(total / WIDTH + NORM_EPSILON)
        scale_ref[n] = row_scale
        proj[0:384] = lax.dot_general(
            wt[0:384], xs[n], (((1,), (1,)), ((), ())), preferred_element_type=F32
        ) * row_scale
        for i in range(2):
            lo = i * HEAD
            wide = [
                jnp.concatenate([cols[k, lo : lo + HEAD]] * 2, axis=1) for k in range(2)
            ]
            qout[i, 0:HEAD, at] = norm_rows(proj[lo : lo + HEAD], wide[0]).astype(BF16)
            kvout[i, HEAD : 2 * HEAD, at] = norm_rows(
                proj[128 + lo : 128 + lo + HEAD], wide[1]
            ).astype(BF16)
            kvout[i, 0:HEAD, at] = proj[256 + lo : 256 + lo + HEAD].astype(BF16)

    def project_conv(n):
        at = pl.ds(pl.multiple_of(n * CHUNK, CHUNK), CHUNK)
        proj[384:768] = lax.dot_general(
            wt[384:768], xs[n], (((1,), (1,)), ((), ())), preferred_element_type=F32
        ) * scale_ref[n]
        outer[:, at] = proj[384:512]
        gated[:, at] = (proj[512:640] * proj[640:768]).astype(BF16)

    def chunk(b, k):
        return kvbuf.at[b, :, pl.ds(pl.multiple_of(k * CHUNK, CHUNK), CHUNK)]

    def arrived(b, k):
        drain(chunk(b, k), kvrecv.at[native(b), k])

    def along(n, b, k, yy):
        piece = chunk(b, k)
        remote(piece, piece, ysend.at[0], kvrecv.at[native(b), k], dev(z, yy, x, c)).start()

    def across(n, b, k):
        piece = chunk(b, k)
        remote(piece, piece, dsend.at[n // 4], kvshare.at[b % 4], sib).start()

    up, down, far = (y + 1) % 4, (y + 3) % 4, (y + 2) % 4
    own_a, own_b = set_a * 4 + y, set_b * 4 + y

    def share_a(n, ys, k):
        across(n, set_a * 4 + ys, k)

    def share_b(n, ys, k):
        @pl.when(c == 1)
        def _():
            across(4 + n, set_b * 4 + ys, k)

    def first_hop(k):
        arrived(own_a, k)
        along(0, own_a, k, up)
        arrived(own_b, k)
        along(1, own_b, k, down)
        along(2, own_b, k, up)
        along(3, own_a, k, down)
        share_a(0, y, k)
        share_b(0, y, k)

    def second_hop(k):
        arrived(set_a * 4 + down, k)
        along(4, set_a * 4 + down, k, up)
        arrived(set_b * 4 + up, k)
        along(5, set_b * 4 + up, k, down)
        share_a(1, down, k)
        share_b(2, up, k)
        arrived(set_b * 4 + down, k)
        share_b(1, down, k)
        arrived(set_a * 4 + up, k)
        share_a(2, up, k)

    def last_hop(k):
        arrived(set_a * 4 + far, k)
        share_a(3, far, k)
        arrived(set_b * 4 + far, k)
        share_b(3, far, k)

    def shared_arrived(ys):
        @pl.when(c == 0)
        def _():
            drain(kvbuf.at[pl.ds(0, 2)], kvshare.at[ys])

        @pl.when(c == 1)
        def _():
            drain(kvbuf.at[0], kvshare.at[ys])

    def w_rows(t, kind):
        return pl.ds(pl.multiple_of(kind * 1024 + t * 128, 128), 128)

    def w_send(n, t, kind, to):
        piece = wbuf.at[w_rows(t, kind)]
        remote(piece, piece, wsend.at[0], wrecv.at[t // 2], to).start()

    def w_across(t):
        piece = wbuf.at[w_rows(t, 0)]
        remote(piece, piece, wsend.at[0], wshare.at[0], sib).start()

    def w_wait(t, kind):
        drain(wbuf.at[w_rows(t, kind)], wrecv.at[t // 2])

    before, after, far_x = left * 2 + c, right * 2 + c, across_x * 2 + c
    near_z = z + 1 - 2 * (z % 2)

    def h_rows(t, half):
        return wbuf.at[pl.ds(pl.multiple_of(1024 + t * 128 + half * 64, 64), 64)]

    def h_send(n, t, to):
        piece = h_rows(t, z % 2)
        remote(piece, piece, hsend.at[0], hrecv.at[t // 2, z % 2], to).start()

    def h_across(n, t, half):
        piece = h_rows(t, half)
        remote(piece, piece, hdsend.at[0], hshare.at[0], sib).start()

    def h_wait(t, half):
        drain(h_rows(t, half), hrecv.at[t // 2, half])

    def w_first():
        out_a.wait()
        out_c.wait()
        h_send(0, tp, dev(z, y, right, c))
        h_send(1, tp, dev(z, y, left, c))
        w_across(tp)
        h_across(0, tp, 0)
        h_across(1, tp, 1)

    def w_second():
        h_wait(before, z % 2)
        h_wait(after, z % 2)

        @pl.when(c == 0)
        def _():
            h_send(2, before, dev(z, y, right, c))

        @pl.when(c == 1)
        def _():
            h_send(2, after, dev(z, y, left, c))

        w_send(0, tp, 0, dev(z, y, right, c))
        w_send(1, tp, 0, dev(z, y, left, c))

    def w_third():
        partner = dev(near_z, y, x, c)
        h_send(3, before, partner)
        h_send(4, after, partner)
        h_across(2, before, z % 2)
        h_across(3, after, z % 2)

    def w_far():
        h_wait(far_x, z % 2)
        h_send(5, far_x, dev(near_z, y, x, c))
        h_across(4, far_x, z % 2)

    def w_fourth():
        w_wait(before, 0)
        w_wait(after, 0)

        @pl.when(c == 0)
        def _():
            w_send(4, before, 0, dev(z, y, right, c))

        @pl.when(c == 1)
        def _():
            w_send(4, after, 0, dev(z, y, left, c))

        w_across(before)
        w_across(after)

    def w_fifth():
        for n, t in enumerate((before, after, far_x)):
            h_wait(t, 1 - z % 2)
            h_across(5 + n, t, 1 - z % 2)

    def gather(n, carry):
        @pl.when(n < 4)
        def _():
            drain(rows(before, n), xrecv.at[before // 2, n])
            piece = rows(before, n, 0)
            remote(piece, piece, xsend.at[0], xrecv.at[before // 2, n], dev(z, y, right, c)).start()
            piece = rows(before, n)
            remote(piece, piece, xdsend.at[0], xshare.at[n], sib).start()
            drain(rows(after, n), xrecv.at[after // 2, n])
            piece = rows(after, n, 1)
            remote(piece, piece, xsend.at[0], xrecv.at[after // 2, n], dev(z, y, left, c)).start()
            piece = rows(after, n)
            remote(piece, piece, xdsend.at[0], xshare.at[n], sib).start()

            @pl.when(n < 2)
            def _():
                send_own(n + 2)

            @pl.when(n == 3)
            def _():
                w_first()

        @pl.when(n > 2)
        def _():
            first_hop(n - 3)

        @pl.when(n > 0)
        def _():
            done = n - 1
            far = across_x * 2 + c
            drain(rows(far, done), xrecv.at[far // 2, done])
            piece = rows(far, done)
            remote(piece, piece, xdsend.at[0], xshare.at[done], sib).start()
            drain(
                xbuf.at[pl.ds(0, 4), pl.ds(pl.multiple_of(done * CHUNK, CHUNK), CHUNK)],
                xshare.at[done],
            )
            project(done)
            z_sends(done)

        return carry

    lax.fori_loop(0, 5, gather, 0)
    second_hop(0)
    project_conv(3)

    @pl.when(sp < 15)
    def _():
        remote(
            gated.at[:, pl.ds(ROWS - 128, 128)], halo, hsem.at[0], hsem.at[1],
            {"sp": jnp.minimum(sp + 1, 15), "tp": tp},
        ).start()

    def mix_conv():
        prior = jnp.concatenate([halo[...], gated[...]], axis=1).astype(F32)
        conv = jnp.concatenate([cols[4]] * 8, axis=1) * prior[:, 128:]
        for tap in range(2):
            moved = pltpu.roll(prior, 2 - tap, axis=1)
            conv = conv + jnp.concatenate([cols[2 + tap]] * 8, axis=1) * moved[:, 128:]
        value = outer[...] * conv
        for i in range(2):
            part = slice(i * HEAD, (i + 1) * HEAD)
            wide = jnp.concatenate([cols[5, part]] * 8, axis=1)
            cstage[part, :] = norm_rows(value[part], wide).astype(BF16)

    def queries_arrived(k):
        at = pl.ds(k * CHUNK, CHUNK)
        for slot in range(2):
            drain(qbuf.at[slot, pl.ds(0, QROWS), at], qrecv.at[slot, k])

    def lay_keys(b, slot, lo=0, hi=ROWS):
        block = jnp.concatenate(
            [kvbuf[b, HEAD:, lo:hi], jnp.zeros((128 - QROWS, hi - lo), BF16)], axis=0
        )
        kaug[slot, lo:hi] = block.T

    def fold(qs, b, s, tile, keys):
        at = pl.ds(tile * TILE, TILE)
        old = m_ref[qs, :, at]
        new = jnp.maximum(old, jnp.max(s, axis=0, keepdims=True))
        p = jnp.exp2(s - new).astype(BF16)
        factor = jnp.exp2(old - new)
        acc_ref[qs, :, at] = acc_ref[qs, :, at] * factor + jnp.dot(
            kvbuf[b, 0:HEAD, 0:keys], p, preferred_element_type=F32
        )
        m_ref[qs, :, at] = new

    def scores(slot, qs, tile, keys=ROWS):
        return jnp.dot(
            kaug[slot, 0:keys, :], qbuf[qs, :, pl.ds(tile * TILE, TILE)],
            preferred_element_type=F32,
        )

    def masked(s, keys):
        key = lax.broadcasted_iota(jnp.int32, (TILE, TILE), 0)
        query = lax.broadcasted_iota(jnp.int32, (TILE, TILE), 1)
        last = jnp.where(key <= query, s[keys - TILE :, :], -1e30)
        if keys == TILE:
            return last
        return jnp.concatenate([s[: keys - TILE, :], last], axis=0)

    def diagonal(tile):
        keys = (tile + 1) * TILE
        for slot, b in enumerate((own_a, own_b)):
            lay_keys(b, slot, tile * TILE, keys)
        for slot, b in enumerate((own_a, own_b)):
            fold(slot, b, masked(scores(slot, slot, tile, keys), keys), tile, keys)

    queries_arrived(0)
    queries_arrived(1)
    diagonal(0)
    first_hop(2)
    w_second()

    def conv_rest(n, carry):
        project_conv(n)
        return carry

    lax.fori_loop(0, 3, conv_rest, 0)
    first_hop(3)
    queries_arrived(2)
    queries_arrived(3)
    diagonal(1)
    second_hop(1)
    w_third()

    @pl.when(sp > 0)
    def _():
        drain(halo, hsem.at[1])

    mix_conv()
    to_rows = pl.ds(pl.multiple_of(1024 + tp * 128, 128), 128)
    local(
        cstage.at[:, pl.ds(pl.multiple_of(tp * 128, 128), 128)], cbuf.at[to_rows], crecv.at[0]
    ).start()
    for step in range(1, 8):
        t = (tp + step) % 8
        remote(
            cstage.at[:, pl.ds(pl.multiple_of(t * 128, 128), 128)], cbuf.at[to_rows],
            csend.at[0], crecv.at[0], {"sp": sp, "tp": t},
        ).start()


    def run(item, count, ahead):
        qs, b = item(0)
        lay_keys(b, 0)
        s_ref[0] = scores(0, qs, 0)

        def body(n, carry):
            ahead(n + 1)
            qs, b = item(n)
            qn, bn = item(jnp.minimum(n + 1, count - 1))
            cur = n % 2
            s_ref[1] = scores(cur, qs, 1)
            fold(qs, b, s_ref[0], 0, ROWS)
            lay_keys(bn, 1 - cur)
            s_ref[0] = scores(1 - cur, qn, 0)
            fold(qs, b, s_ref[1], 1, ROWS)
            return carry

        lax.fori_loop(0, count, body, 0)

    def pick_far(n, ys, earlier):
        early = jnp.where(c == 0, earlier, 2 + earlier)
        k = n - early
        early_z = jnp.where(c == 0, set_a, n)
        late_z = jnp.where(c == 0, k, jnp.where(k == 0, 0, set_a))
        qs = jnp.where(k < 0, c, 1 - c)
        return qs, jnp.where(k < 0, early_z, late_z) * 4 + ys

    def pick_near(n, ys, earlier):
        k = n - 1 - 2 * earlier
        shared_q = jnp.where((c == 1) & (k == 0), 0, 1)
        shared_z = jnp.where(c == 0, 1 + k, 0)
        qs = jnp.where(k >= 0, shared_q, jnp.where(n == 1, 0, 1))
        zs = jnp.where(k >= 0, shared_z, jnp.where(n == 2, set_b, set_a))
        return qs, zs * 4 + ys

    def send_heads(slot):
        stage[slot] = norm_rows(acc_ref[slot], gbuf[slot][:, 0:1]).astype(BF16)
        head = x * 4 + z
        dst = cbuf.at[pl.ds(pl.multiple_of(head * HEAD, HEAD), HEAD)]
        zt = jnp.where(slot == 0, set_a, set_b)
        for step in range(8):
            t = (tp + step) % 8
            piece = stage.at[slot, :, pl.ds(pl.multiple_of(t * 128, 128), 128)]
            to = {"sp": zt * 4 + y, "tp": t}
            if step:
                remote(piece, dst, osend.at[slot], arecv.at[0], to).start()
                continue

            @pl.when(zt == z)
            def _():
                local(piece, dst, arecv.at[0]).start()

            @pl.when(zt != z)
            def _():
                remote(piece, dst, osend.at[2 + slot], arecv.at[0], to).start()

    for slot in range(2):
        drain(gbuf.at[slot], grecv.at[slot])
    shared_arrived(y)
    run(lambda n: pick_near(n, y, 0), 3, lambda n: None)
    second_hop(2)
    second_hop(3)
    w_far()

    from_down = jnp.where(down < y, 1, 0)
    from_up = jnp.where(up < y, 1, 0)
    from_far = jnp.where(far < y, 1, 0)
    at_up = 3 + 2 * from_down
    at_far = at_up + 3 + 2 * from_up
    first_far = jnp.where(c == 0, from_far, 2 + from_far)
    last_item = at_far + 2 + 2 * from_far

    def item(n):
        ys = jnp.where(n < at_up, down, jnp.where(n < at_far, up, far))
        earlier = jnp.where(n < at_up, from_down, jnp.where(n < at_far, from_up, from_far))
        start = jnp.where(n < at_up, 0, jnp.where(n < at_far, at_up, at_far))
        late = pick_far(n - at_far, far, from_far)
        soon = pick_near(n - start, ys, earlier)
        return tuple(jnp.where(n < at_far, a, b) for a, b in zip(soon, late))

    def ahead(n):
        @pl.when(n == 1 + 2 * from_down)
        def _():
            shared_arrived(down)

        @pl.when(n == 2)
        def _():
            last_hop(0)
            last_hop(1)

        @pl.when((n == last_item) & (y > 1))
        def _():
            w_fifth()

        @pl.when(n == at_far + first_far + 1)
        def _():
            send_heads(c)

        @pl.when(n == jnp.where(y == 0, 5, 7))
        def _():
            w_fourth()

        @pl.when(n == at_up)
        def _():
            last_hop(2)
            last_hop(3)
            shared_arrived(up)

        @pl.when(n == at_far)
        def _():
            shared_arrived(far)

    run(item, at_far + 3 + 2 * from_far, ahead)
    send_heads(1 - c)

    @pl.when(y < 2)
    def _():
        w_fifth()

    w_wait(far_x, 0)
    w_across(far_x)
    drain(wbuf.at[pl.ds(0, 512)], hshare.at[0])
    drain(cbuf.at[pl.ds(1024, 1024)], crecv.at[0])

    def product(lo, n):
        at = pl.ds(n * TILE, TILE)
        return jnp.dot(
            ct[:, lo : lo + 1024], wbuf[lo : lo + 1024, at], preferred_element_type=F32
        )

    def conv_part(n, carry):
        oacc[:, pl.ds(n * TILE, TILE)] = product(1024, n)
        return carry

    ct[:, 1024:] = cbuf[1024:, :].T
    for n in range(WIDTH // TILE):
        conv_part(n, 0)
    drain(wbuf.at[pl.ds(0, 512)], wshare.at[0])
    drain(cbuf.at[pl.ds(0, 1024)], arecv.at[0])

    def attn_part(n, carry):
        at = pl.ds(n * TILE, TILE)
        out_ref[:, at] = (oacc[:, at] + product(0, n)).astype(BF16)
        return carry

    ct[:, :1024] = cbuf[:1024, :].T
    for n in range(WIDTH // TILE):
        attn_part(n, 0)

    drain(xbuf.at[pl.ds(0, 3)], xsend.at[0])
    drain(xbuf.at[pl.ds(0, 4)], xdsend.at[0])
    drain(kvbuf.at[pl.ds(0, 6)], ysend.at[0])
    drain(kvbuf.at[pl.ds(0, 4)], dsend.at[0])

    @pl.when(c == 1)
    def _():
        drain(kvbuf.at[pl.ds(0, 4)], dsend.at[1])

    for i in range(2):
        zt = 2 * c + i
        own = (zt == z) & (zc == c)

        @pl.when(jnp.logical_not(own))
        def _():
            drain(gout.at[i], gsend.at[i])
            drain(kvout.at[i], zsend.at[i, 0])
            drain(qout.at[i], zsend.at[i, 1])

    @pl.when(sp < 15)
    def _():
        drain(halo, hsem.at[0])

    drain(wbuf.at[pl.ds(0, 896)], wsend.at[0])
    drain(wbuf.at[pl.ds(0, 512)], hdsend.at[0])
    drain(wbuf.at[pl.ds(0, 384)], hsend.at[0])
    drain(cbuf.at[pl.ds(0, 896)], csend.at[0])
    for slot in range(2):
        zt = jnp.where(slot == 0, set_a, set_b)
        drain(stage.at[slot, :, pl.ds(0, 896)], osend.at[slot])

        @pl.when(zt != z)
        def _():
            drain(stage.at[slot, :, pl.ds(0, 128)], osend.at[2 + slot])


def store_kernel(rows, out, sem):
    copy = pltpu.make_async_copy(rows, out, sem)
    copy.start()
    copy.wait()


def per_device(
    tokens, mix_gain, query_weight, key_weight, value_weight, outer_gate_weight,
    inner_gate_weight, conv_input_weight, query_gain, key_gain, gate_totals, conv_taps,
    attn_out_gain, conv_out_gain, attn_out_weight, conv_out_weight,
):
    DMA = pltpu.SemaphoreType.DMA
    far = pl.BlockSpec(memory_space=pl.ANY)
    near = pl.BlockSpec(memory_space=VMEM)
    rows = pl.pallas_call(
        layer_kernel,
        out_shape=pltpu.VMEM((128, WIDTH), BF16),
        in_specs=[far] * 16,
        out_specs=near,
        scratch_shapes=[
            VMEM((1, WIDTH), F32),
            VMEM((1, HEAD), F32),
            VMEM((1, HEAD), F32),
            VMEM((2, ROWS), F32),
            VMEM((3, 128), F32),
            VMEM((1, 128), F32),
            VMEM((1, 128), F32),
            VMEM((8, ROWS, FEATURES), BF16),
            VMEM((6, WIDTH, 128), BF16),
            VMEM((768, WIDTH), BF16),
            VMEM((4, CHUNK, WIDTH), BF16),
            VMEM((4, 1, CHUNK), F32),
            VMEM((768, CHUNK), F32),
            VMEM((128, ROWS), F32),
            VMEM((128, ROWS), BF16),
            VMEM((128, 128), BF16),
            VMEM((2, QROWS, ROWS), BF16),
            VMEM((2, KVROWS, ROWS), BF16),
            VMEM((2, HEAD, 128), F32),
            VMEM((6, 128, 128), F32),
            VMEM((2, 128, ROWS), BF16),
            VMEM((16, KVROWS, ROWS), BF16),
            VMEM((2, HEAD, 128), F32),
            VMEM((2, ROWS, 128), BF16),
            VMEM((2, ROWS, TILE), F32),
            VMEM((2, 1, ROWS), F32),
            VMEM((2, HEAD, ROWS), F32),
            VMEM((2, HEAD, ROWS), BF16),
            VMEM((128, ROWS), BF16),
            VMEM((WIDTH, WIDTH), BF16),
            VMEM((WIDTH, 128), BF16),
            VMEM((128, WIDTH), BF16),
            VMEM((128, WIDTH), F32),
            DMA((16,)), DMA((1,)), DMA((1,)), DMA((4, 4)), DMA((4,)), DMA((2,)), DMA((2, 2)),
            DMA((2,)), DMA((1,)), DMA((2,)), DMA((4,)), DMA((1,)), DMA((1,)), DMA((1,)), DMA((1,)),
            DMA((2, 4)), DMA((8, 4)), DMA((4,)), DMA((2,)), DMA((4,)), DMA((1,)), DMA((4, 2)),
            DMA((1,)), DMA((1,)), DMA((1,)),
        ],
        compiler_params=pltpu.CompilerParams(
            collective_id=1, has_side_effects=True, vmem_limit_bytes=56 * 2**20
        ),
        name="layer",
    )(
        tokens, mix_gain.reshape(1, WIDTH), query_weight, key_weight, value_weight,
        outer_gate_weight, inner_gate_weight, conv_input_weight, query_gain.reshape(1, HEAD),
        key_gain.reshape(1, HEAD), gate_totals.T, conv_taps, attn_out_gain.reshape(1, 128),
        conv_out_gain.reshape(1, 128), attn_out_weight, conv_out_weight,
    )
    return pl.pallas_call(
        store_kernel,
        out_shape=jax.ShapeDtypeStruct((128, WIDTH), BF16),
        in_specs=[near],
        out_specs=far,
        scratch_shapes=[DMA],
        name="store",
    )(pltpu.with_memory_space_constraint(rows, pltpu.VMEM))


def solution(mesh):
    placed = (
        P("sp", "tp"), P(), P(None, "tp"), P(None, "tp"), P(None, "tp"), P(None, "tp"),
        P(None, "tp"), P(None, "tp"), P(), P(), P("sp", "tp"), P(None, "tp"), P("tp"),
        P("tp"), P("tp", None), P("tp", None),
    )
    return jax.shard_map(
        per_device, mesh=mesh, in_specs=placed, out_specs=P(("sp", "tp"), None), check_vma=False
    )
```

```python
import math

import jax
import jax.numpy as jnp
from jax import lax
from jax.experimental import pallas as pl
from jax.experimental.pallas import tpu as pltpu
from jax.sharding import PartitionSpec as P

NORM_EPSILON = 1e-06
MESH = pl.DeviceIdType.MESH
VMEM = pltpu.VMEM
LOG2E = math.log2(math.e)
WIDTH = 2048
ROWS = 1024
CHUNK = 256
FEATURES = 256
HEAD = 64
QROWS = 80
KVROWS = 144
TILE = 512
F32 = jnp.float32
BF16 = jnp.bfloat16


def column(row):
    return jnp.broadcast_to(row, (128, 128)).T


def norm_rows(values, gain):
    scale = lax.rsqrt(jnp.mean(values * values, axis=0, keepdims=True) + NORM_EPSILON)
    return values * scale * gain


def layer_kernel(
    tokens, mix_in, wq, wk, wv, wo, wi, wx, qgain_in, kgain_in, gates_in, taps_in, again_in,
    cgain_in, wa, wc, out_ref, mix, qgain, kgain, gates, taps, again, cgain,
    xbuf, wtmp, wt, xs, scale_ref, proj, outer, gated, halo, qout, kvout, gout, cols,
    qbuf, kvbuf, gbuf, kaug, s_ref, m_ref, acc_ref, stage, cstage, wbuf, cbuf, ct, oacc,
    lsem, xsend, xdsend, xrecv, xshare, hsem, zsend, gsend, ysend, dsend, osend, csend, wsend,
    hsend, hdsend, qrecv, kvrecv, kvshare, grecv, wrecv, wshare, hrecv, hshare, arecv, crecv,
):
    sp = lax.axis_index("sp")
    tp = lax.axis_index("tp")
    z, y = sp // 4, sp % 4
    x, c = tp // 2, tp % 2
    zc = jnp.where((z == 1) | (z == 2), 1, 0)
    set_a = c
    set_b = 3 - c

    def dev(zz, yy, xx, cc):
        return {"sp": zz * 4 + yy, "tp": xx * 2 + cc}

    def local(src, dst, sem):
        return pltpu.make_async_copy(src, dst, sem)

    def remote(src, dst, send, recv, to):
        return pltpu.make_async_remote_copy(
            src_ref=src, dst_ref=dst, send_sem=send, recv_sem=recv, device_id=to,
            device_id_type=MESH,
        )

    def drain(ref, sem):
        pltpu.make_async_copy(ref, ref, sem).wait()

    mine = local(tokens, xbuf.at[tp], lsem.at[0])
    mine.start()
    barrier = pltpu.get_barrier_semaphore()
    columns = [((z + step) % 4) * 4 + y for step in range(4)]
    ranks = [(tp + step) % 8 for step in range(8)]
    for n in range(1, 32):
        pl.semaphore_signal(
            barrier, inc=1, device_id={"sp": columns[n // 8], "tp": ranks[n % 8]},
            device_id_type=MESH,
        )
    for step in (1, 3):
        pl.semaphore_signal(
            barrier, inc=1, device_id=dev(z, (y + step) % 4, x, c), device_id_type=MESH
        )
    for step in (1, 15):
        pl.semaphore_signal(
            barrier, inc=1, device_id={"sp": (sp + step) % 16, "tp": tp}, device_id_type=MESH
        )
    weights = [
        local(w, wtmp.at[n], lsem.at[1 + n]) for n, w in enumerate((wq, wk, wv, wo, wi, wx))
    ]
    own_wa = pl.ds(pl.multiple_of(tp * 128, 128), 128)
    own_wc = pl.ds(pl.multiple_of(1024 + tp * 128, 128), 128)
    out_a = local(wa, wbuf.at[own_wa], lsem.at[7])
    out_c = local(wc, wbuf.at[own_wc], lsem.at[8])
    smalls = [
        local(src, dst, lsem.at[9 + n])
        for n, (src, dst) in enumerate((
            (qgain_in, qgain), (kgain_in, kgain), (gates_in, gates), (taps_in, taps),
            (again_in, again), (cgain_in, cgain), (mix_in, mix),
        ))
    ]
    for small in smalls:
        small.start()

    for w in weights:
        w.start()
    out_a.start()
    out_c.start()
    mine.wait()
    pl.semaphore_wait(barrier, 35)

    right, left, across_x = (x + 1) % 4, (x + 3) % 4, (x + 2) % 4
    sib = dev(z, y, x, 1 - c)

    def rows(t, n, half=None):
        if half is None:
            return xbuf.at[t, pl.ds(pl.multiple_of(n * CHUNK, CHUNK), CHUNK)]
        return xbuf.at[t, pl.ds(pl.multiple_of(n * CHUNK + half * 128, 128), 128)]

    def send_own(n):
        piece = rows(tp, n)
        remote(piece, piece, xsend.at[0], xrecv.at[tp // 2, n], dev(z, y, right, c)).start()
        remote(piece, piece, xsend.at[0], xrecv.at[tp // 2, n], dev(z, y, left, c)).start()
        remote(piece, piece, xdsend.at[0], xshare.at[n], sib).start()

    send_own(0)
    send_own(1)

    for small in smalls:
        small.wait()
    for n, row in enumerate((qgain, kgain)):
        both = jnp.concatenate([row[...], row[...]], axis=1)
        if n == 0:
            both = both * (LOG2E * HEAD**-0.5)
        cols[n] = column(both)
    for n in range(3):
        cols[2 + n] = column(taps[n : n + 1, :])
    cols[5] = column(cgain[...])
    out_gain = column(again[...])
    for i in range(2):
        gout[i] = out_gain[i * HEAD : (i + 1) * HEAD]
    spot = lax.broadcasted_iota(jnp.int32, (16, ROWS), 0)
    for i in range(2):
        g = gates[i : i + 1, :] * LOG2E
        hi = g.astype(BF16).astype(F32)
        mid = (g - hi).astype(BF16).astype(F32)
        low = g - hi - mid
        one = jnp.where(spot < 3, 1.0, 0.0)
        parts = jnp.where(spot == 3, hi, jnp.where(spot == 4, mid, jnp.where(spot == 5, low, one)))
        qout[i, HEAD:, :] = parts.astype(BF16)
        one = jnp.where((spot > 2) & (spot < 6), 1.0, 0.0)
        parts = jnp.where(spot == 0, -hi, jnp.where(spot == 1, -mid, jnp.where(spot == 2, -low, one)))
        kvout[i, 2 * HEAD :, :] = parts.astype(BF16)
    for n, w in enumerate(weights):
        w.wait()
        for k in range(4):
            wt[n * 128 : (n + 1) * 128, k * 512 : (k + 1) * 512] = wtmp[
                n, k * 512 : (k + 1) * 512, :
            ].T

    for slot in range(2):
        qbuf[slot, QROWS:, :] = jnp.zeros((128 - QROWS, ROWS), BF16)
    m_ref[...] = jnp.full_like(m_ref, -1e30)
    acc_ref[...] = jnp.zeros_like(acc_ref)

    @pl.when(sp == 0)
    def _():
        halo[...] = jnp.zeros_like(halo)

    qslot = z // 2

    def native(b):
        return jnp.where(b < 8, 0, 4) + b % 4

    def z_sends(n):
        at = pl.ds(pl.multiple_of(n * CHUNK, CHUNK), CHUNK)
        for k in range(2):
            for i in range(2):
                zt = 2 * c + i
                own = (zt == z) & (zc == c)
                src, dst, recv = (
                    (kvout.at[i, :, at], kvbuf.at[sp, :, at], kvrecv.at[native(sp), n]),
                    (qout.at[i, :, at], qbuf.at[qslot, pl.ds(0, QROWS), at], qrecv.at[qslot, n]),
                )[k]

                @pl.when(own)
                def _():
                    local(src, dst, recv).start()

                @pl.when(jnp.logical_not(own))
                def _():
                    remote(src, dst, zsend.at[i, k], recv, dev(zt, y, x, zc)).start()

    for i in range(2):
        zt = 2 * c + i
        own = (zt == z) & (zc == c)

        @pl.when(own)
        def _():
            local(gout.at[i], gbuf.at[qslot], grecv.at[qslot]).start()

        @pl.when(jnp.logical_not(own))
        def _():
            remote(
                gout.at[i], gbuf.at[qslot], gsend.at[i], grecv.at[qslot], dev(zt, y, x, zc)
            ).start()

    def project(n):
        at = pl.ds(pl.multiple_of(n * CHUNK, CHUNK), CHUNK)
        squares = jnp.zeros((CHUNK, 128), F32)
        for t in range(8):
            piece = xbuf[t, at, :].astype(F32)
            squares = squares + piece[:, :128] * piece[:, :128] + piece[:, 128:] * piece[:, 128:]
            lanes = slice(t * FEATURES, (t + 1) * FEATURES)
            xs[n, :, lanes] = (piece * mix[:, lanes]).astype(BF16)
        total = jnp.sum(squares.T, axis=0, keepdims=True)
        row_scale = lax.rsqrt(total / WIDTH + NORM_EPSILON)
        scale_ref[n] = row_scale
        proj[0:384] = lax.dot_general(
            wt[0:384], xs[n], (((1,), (1,)), ((), ())), preferred_element_type=F32
        ) * row_scale
        for i in range(2):
            lo = i * HEAD
            wide = [
                jnp.concatenate([cols[k, lo : lo + HEAD]] * 2, axis=1) for k in range(2)
            ]
            qout[i, 0:HEAD, at] = norm_rows(proj[lo : lo + HEAD], wide[0]).astype(BF16)
            kvout[i, HEAD : 2 * HEAD, at] = norm_rows(
                proj[128 + lo : 128 + lo + HEAD], wide[1]
            ).astype(BF16)
            kvout[i, 0:HEAD, at] = proj[256 + lo : 256 + lo + HEAD].astype(BF16)

    def project_conv(n):
        at = pl.ds(pl.multiple_of(n * CHUNK, CHUNK), CHUNK)
        proj[384:768] = lax.dot_general(
            wt[384:768], xs[n], (((1,), (1,)), ((), ())), preferred_element_type=F32
        ) * scale_ref[n]
        outer[:, at] = proj[384:512]
        gated[:, at] = (proj[512:640] * proj[640:768]).astype(BF16)

    def chunk(b, k):
        return kvbuf.at[b, :, pl.ds(pl.multiple_of(k * CHUNK, CHUNK), CHUNK)]

    def arrived(b, k):
        drain(chunk(b, k), kvrecv.at[native(b), k])

    def along(n, b, k, yy):
        piece = chunk(b, k)
        remote(piece, piece, ysend.at[0], kvrecv.at[native(b), k], dev(z, yy, x, c)).start()

    def across(n, b, k):
        piece = chunk(b, k)
        remote(piece, piece, dsend.at[n // 4], kvshare.at[b % 4], sib).start()

    up, down, far = (y + 1) % 4, (y + 3) % 4, (y + 2) % 4
    own_a, own_b = set_a * 4 + y, set_b * 4 + y

    def share_a(n, ys, k):
        across(n, set_a * 4 + ys, k)

    def share_b(n, ys, k):
        @pl.when(c == 1)
        def _():
            across(4 + n, set_b * 4 + ys, k)

    def first_hop(k):
        arrived(own_a, k)
        along(0, own_a, k, up)
        arrived(own_b, k)
        along(1, own_b, k, down)
        along(2, own_b, k, up)
        along(3, own_a, k, down)
        share_a(0, y, k)
        share_b(0, y, k)

    def second_hop(k):
        arrived(set_a * 4 + down, k)
        along(4, set_a * 4 + down, k, up)
        arrived(set_b * 4 + up, k)
        along(5, set_b * 4 + up, k, down)
        share_a(1, down, k)
        share_b(2, up, k)
        arrived(set_b * 4 + down, k)
        share_b(1, down, k)
        arrived(set_a * 4 + up, k)
        share_a(2, up, k)

    def last_hop(k):
        arrived(set_a * 4 + far, k)
        share_a(3, far, k)
        arrived(set_b * 4 + far, k)
        share_b(3, far, k)

    def shared_arrived(ys):
        @pl.when(c == 0)
        def _():
            drain(kvbuf.at[pl.ds(0, 2)], kvshare.at[ys])

        @pl.when(c == 1)
        def _():
            drain(kvbuf.at[0], kvshare.at[ys])

    def w_rows(t, kind):
        return pl.ds(pl.multiple_of(kind * 1024 + t * 128, 128), 128)

    def w_send(n, t, kind, to):
        piece = wbuf.at[w_rows(t, kind)]
        remote(piece, piece, wsend.at[0], wrecv.at[t // 2], to).start()

    def w_across(t):
        piece = wbuf.at[w_rows(t, 0)]
        remote(piece, piece, wsend.at[0], wshare.at[0], sib).start()

    def w_wait(t, kind):
        drain(wbuf.at[w_rows(t, kind)], wrecv.at[t // 2])

    before, after, far_x = left * 2 + c, right * 2 + c, across_x * 2 + c
    near_z = z + 1 - 2 * (z % 2)

    def h_rows(t, half):
        return wbuf.at[pl.ds(pl.multiple_of(1024 + t * 128 + half * 64, 64), 64)]

    def h_send(n, t, to):
        piece = h_rows(t, z % 2)
        remote(piece, piece, hsend.at[0], hrecv.at[t // 2, z % 2], to).start()

    def h_across(n, t, half):
        piece = h_rows(t, half)
        remote(piece, piece, hdsend.at[0], hshare.at[0], sib).start()

    def h_wait(t, half):
        drain(h_rows(t, half), hrecv.at[t // 2, half])

    def w_first():
        out_a.wait()
        out_c.wait()
        h_send(0, tp, dev(z, y, right, c))
        h_send(1, tp, dev(z, y, left, c))
        w_across(tp)
        h_across(0, tp, 0)
        h_across(1, tp, 1)

    def w_second():
        h_wait(before, z % 2)
        h_wait(after, z % 2)

        @pl.when(c == 0)
        def _():
            h_send(2, before, dev(z, y, right, c))

        @pl.when(c == 1)
        def _():
            h_send(2, after, dev(z, y, left, c))

        w_send(0, tp, 0, dev(z, y, right, c))
        w_send(1, tp, 0, dev(z, y, left, c))

    def w_third():
        partner = dev(near_z, y, x, c)
        h_send(3, before, partner)
        h_send(4, after, partner)
        h_across(2, before, z % 2)
        h_across(3, after, z % 2)

    def w_far():
        h_wait(far_x, z % 2)
        h_send(5, far_x, dev(near_z, y, x, c))
        h_across(4, far_x, z % 2)

    def w_fourth():
        w_wait(before, 0)
        w_wait(after, 0)

        @pl.when(c == 0)
        def _():
            w_send(4, before, 0, dev(z, y, right, c))

        @pl.when(c == 1)
        def _():
            w_send(4, after, 0, dev(z, y, left, c))

        w_across(before)
        w_across(after)

    def w_fifth():
        for n, t in enumerate((before, after, far_x)):
            h_wait(t, 1 - z % 2)
            h_across(5 + n, t, 1 - z % 2)

    def gather(n, carry):
        @pl.when(n < 4)
        def _():
            drain(rows(before, n), xrecv.at[before // 2, n])
            piece = rows(before, n, 0)
            remote(piece, piece, xsend.at[0], xrecv.at[before // 2, n], dev(z, y, right, c)).start()
            piece = rows(before, n)
            remote(piece, piece, xdsend.at[0], xshare.at[n], sib).start()
            drain(rows(after, n), xrecv.at[after // 2, n])
            piece = rows(after, n, 1)
            remote(piece, piece, xsend.at[0], xrecv.at[after // 2, n], dev(z, y, left, c)).start()
            piece = rows(after, n)
            remote(piece, piece, xdsend.at[0], xshare.at[n], sib).start()

            @pl.when(n < 2)
            def _():
                send_own(n + 2)

            @pl.when(n == 3)
            def _():
                w_first()

        @pl.when(n > 2)
        def _():
            first_hop(n - 3)

        @pl.when(n > 0)
        def _():
            done = n - 1
            far = across_x * 2 + c
            drain(rows(far, done), xrecv.at[far // 2, done])
            piece = rows(far, done)
            remote(piece, piece, xdsend.at[0], xshare.at[done], sib).start()
            drain(
                xbuf.at[pl.ds(0, 4), pl.ds(pl.multiple_of(done * CHUNK, CHUNK), CHUNK)],
                xshare.at[done],
            )
            project(done)
            z_sends(done)

        return carry

    lax.fori_loop(0, 5, gather, 0)
    second_hop(0)
    project_conv(3)

    @pl.when(sp < 15)
    def _():
        remote(
            gated.at[:, pl.ds(ROWS - 128, 128)], halo, hsem.at[0], hsem.at[1],
            {"sp": jnp.minimum(sp + 1, 15), "tp": tp},
        ).start()

    def mix_conv():
        prior = jnp.concatenate([halo[...], gated[...]], axis=1).astype(F32)
        conv = jnp.concatenate([cols[4]] * 8, axis=1) * prior[:, 128:]
        for tap in range(2):
            moved = pltpu.roll(prior, 2 - tap, axis=1)
            conv = conv + jnp.concatenate([cols[2 + tap]] * 8, axis=1) * moved[:, 128:]
        value = outer[...] * conv
        for i in range(2):
            part = slice(i * HEAD, (i + 1) * HEAD)
            wide = jnp.concatenate([cols[5, part]] * 8, axis=1)
            cstage[part, :] = norm_rows(value[part], wide).astype(BF16)

    def queries_arrived(k):
        at = pl.ds(k * CHUNK, CHUNK)
        for slot in range(2):
            drain(qbuf.at[slot, pl.ds(0, QROWS), at], qrecv.at[slot, k])

    def lay_keys(b, slot, lo=0, hi=ROWS):
        block = jnp.concatenate(
            [kvbuf[b, HEAD:, lo:hi], jnp.zeros((128 - QROWS, hi - lo), BF16)], axis=0
        )
        kaug[slot, lo:hi] = block.T

    def fold(qs, b, s, tile, keys):
        at = pl.ds(tile * TILE, TILE)
        old = m_ref[qs, :, at]
        new = jnp.maximum(old, jnp.max(s, axis=0, keepdims=True))
        p = jnp.exp2(s - new).astype(BF16)
        factor = jnp.exp2(old - new)
        acc_ref[qs, :, at] = acc_ref[qs, :, at] * factor + jnp.dot(
            kvbuf[b, 0:HEAD, 0:keys], p, preferred_element_type=F32
        )
        m_ref[qs, :, at] = new

    def scores(slot, qs, tile, keys=ROWS):
        return jnp.dot(
            kaug[slot, 0:keys, :], qbuf[qs, :, pl.ds(tile * TILE, TILE)],
            preferred_element_type=F32,
        )

    def masked(s, keys):
        key = lax.broadcasted_iota(jnp.int32, (TILE, TILE), 0)
        query = lax.broadcasted_iota(jnp.int32, (TILE, TILE), 1)
        last = jnp.where(key <= query, s[keys - TILE :, :], -1e30)
        if keys == TILE:
            return last
        return jnp.concatenate([s[: keys - TILE, :], last], axis=0)

    def diagonal(tile):
        keys = (tile + 1) * TILE
        for slot, b in enumerate((own_a, own_b)):
            lay_keys(b, slot, tile * TILE, keys)
        for slot, b in enumerate((own_a, own_b)):
            fold(slot, b, masked(scores(slot, slot, tile, keys), keys), tile, keys)

    queries_arrived(0)
    queries_arrived(1)
    diagonal(0)
    first_hop(2)
    w_second()

    def conv_rest(n, carry):
        project_conv(n)
        return carry

    lax.fori_loop(0, 3, conv_rest, 0)
    first_hop(3)
    queries_arrived(2)
    queries_arrived(3)
    diagonal(1)
    second_hop(1)
    w_third()

    @pl.when(sp > 0)
    def _():
        drain(halo, hsem.at[1])

    mix_conv()
    to_rows = pl.ds(pl.multiple_of(1024 + tp * 128, 128), 128)
    local(
        cstage.at[:, pl.ds(pl.multiple_of(tp * 128, 128), 128)], cbuf.at[to_rows], crecv.at[0]
    ).start()
    for step in range(1, 8):
        t = (tp + step) % 8
        remote(
            cstage.at[:, pl.ds(pl.multiple_of(t * 128, 128), 128)], cbuf.at[to_rows],
            csend.at[0], crecv.at[0], {"sp": sp, "tp": t},
        ).start()


    def run(item, count, ahead):
        qs, b = item(0)
        lay_keys(b, 0)
        s_ref[0] = scores(0, qs, 0)

        def body(n, carry):
            ahead(n + 1)
            qs, b = item(n)
            qn, bn = item(jnp.minimum(n + 1, count - 1))
            cur = n % 2
            s_ref[1] = scores(cur, qs, 1)
            fold(qs, b, s_ref[0], 0, ROWS)
            lay_keys(bn, 1 - cur)
            s_ref[0] = scores(1 - cur, qn, 0)
            fold(qs, b, s_ref[1], 1, ROWS)
            return carry

        lax.fori_loop(0, count, body, 0)

    def pick_far(n, ys, earlier):
        early = jnp.where(c == 0, earlier, 2 + earlier)
        k = n - early
        early_z = jnp.where(c == 0, set_a, n)
        late_z = jnp.where(c == 0, k, jnp.where(k == 0, 0, set_a))
        qs = jnp.where(k < 0, c, 1 - c)
        return qs, jnp.where(k < 0, early_z, late_z) * 4 + ys

    def pick_near(n, ys, earlier):
        k = n - 1 - 2 * earlier
        shared_q = jnp.where((c == 1) & (k == 0), 0, 1)
        shared_z = jnp.where(c == 0, 1 + k, 0)
        qs = jnp.where(k >= 0, shared_q, jnp.where(n == 1, 0, 1))
        zs = jnp.where(k >= 0, shared_z, jnp.where(n == 2, set_b, set_a))
        return qs, zs * 4 + ys

    def send_heads(slot):
        stage[slot] = norm_rows(acc_ref[slot], gbuf[slot][:, 0:1]).astype(BF16)
        head = x * 4 + z
        dst = cbuf.at[pl.ds(pl.multiple_of(head * HEAD, HEAD), HEAD)]
        zt = jnp.where(slot == 0, set_a, set_b)
        for step in range(8):
            t = (tp + step) % 8
            piece = stage.at[slot, :, pl.ds(pl.multiple_of(t * 128, 128), 128)]
            to = {"sp": zt * 4 + y, "tp": t}
            if step:
                remote(piece, dst, osend.at[slot], arecv.at[0], to).start()
                continue

            @pl.when(zt == z)
            def _():
                local(piece, dst, arecv.at[0]).start()

            @pl.when(zt != z)
            def _():
                remote(piece, dst, osend.at[2 + slot], arecv.at[0], to).start()

    for slot in range(2):
        drain(gbuf.at[slot], grecv.at[slot])
    shared_arrived(y)
    run(lambda n: pick_near(n, y, 0), 3, lambda n: None)
    second_hop(2)
    second_hop(3)
    w_far()

    from_down = jnp.where(down < y, 1, 0)
    from_up = jnp.where(up < y, 1, 0)
    from_far = jnp.where(far < y, 1, 0)
    at_up = 3 + 2 * from_down
    at_far = at_up + 3 + 2 * from_up
    first_far = jnp.where(c == 0, from_far, 2 + from_far)
    last_item = at_far + 2 + 2 * from_far

    def item(n):
        ys = jnp.where(n < at_up, down, jnp.where(n < at_far, up, far))
        earlier = jnp.where(n < at_up, from_down, jnp.where(n < at_far, from_up, from_far))
        start = jnp.where(n < at_up, 0, jnp.where(n < at_far, at_up, at_far))
        late = pick_far(n - at_far, far, from_far)
        soon = pick_near(n - start, ys, earlier)
        return tuple(jnp.where(n < at_far, a, b) for a, b in zip(soon, late))

    def ahead(n):
        @pl.when(n == 1 + 2 * from_down)
        def _():
            shared_arrived(down)

        @pl.when(n == 2)
        def _():
            last_hop(0)
            last_hop(1)

        @pl.when((n == last_item) & (y > 1))
        def _():
            w_fifth()

        @pl.when(n == at_far + first_far + 1)
        def _():
            send_heads(c)

        @pl.when(n == jnp.where(y == 0, 5, 7))
        def _():
            w_fourth()

        @pl.when(n == at_up)
        def _():
            last_hop(2)
            last_hop(3)
            shared_arrived(up)

        @pl.when(n == at_far)
        def _():
            shared_arrived(far)

    run(item, at_far + 3 + 2 * from_far, ahead)
    send_heads(1 - c)

    @pl.when(y < 2)
    def _():
        w_fifth()

    w_wait(far_x, 0)
    w_across(far_x)
    drain(wbuf.at[pl.ds(0, 512)], hshare.at[0])
    drain(cbuf.at[pl.ds(1024, 1024)], crecv.at[0])

    def product(lo, n):
        at = pl.ds(n * TILE, TILE)
        return jnp.dot(
            ct[:, lo : lo + 1024], wbuf[lo : lo + 1024, at], preferred_element_type=F32
        )

    def conv_part(n, carry):
        oacc[:, pl.ds(n * TILE, TILE)] = product(1024, n)
        return carry

    ct[:, 1024:] = cbuf[1024:, :].T
    for n in range(WIDTH // TILE):
        conv_part(n, 0)
    drain(wbuf.at[pl.ds(0, 512)], wshare.at[0])
    drain(cbuf.at[pl.ds(0, 1024)], arecv.at[0])

    def attn_part(n, carry):
        at = pl.ds(n * TILE, TILE)
        out_ref[:, at] = (oacc[:, at] + product(0, n)).astype(BF16)
        return carry

    ct[:, :1024] = cbuf[:1024, :].T
    for n in range(WIDTH // TILE):
        attn_part(n, 0)

    drain(xbuf.at[pl.ds(0, 3)], xsend.at[0])
    drain(xbuf.at[pl.ds(0, 4)], xdsend.at[0])
    drain(kvbuf.at[pl.ds(0, 6)], ysend.at[0])
    drain(kvbuf.at[pl.ds(0, 4)], dsend.at[0])

    @pl.when(c == 1)
    def _():
        drain(kvbuf.at[pl.ds(0, 4)], dsend.at[1])

    for i in range(2):
        zt = 2 * c + i
        own = (zt == z) & (zc == c)

        @pl.when(jnp.logical_not(own))
        def _():
            drain(gout.at[i], gsend.at[i])
            drain(kvout.at[i], zsend.at[i, 0])
            drain(qout.at[i], zsend.at[i, 1])

    @pl.when(sp < 15)
    def _():
        drain(halo, hsem.at[0])

    drain(wbuf.at[pl.ds(0, 896)], wsend.at[0])
    drain(wbuf.at[pl.ds(0, 512)], hdsend.at[0])
    drain(wbuf.at[pl.ds(0, 384)], hsend.at[0])
    drain(cbuf.at[pl.ds(0, 896)], csend.at[0])
    for slot in range(2):
        zt = jnp.where(slot == 0, set_a, set_b)
        drain(stage.at[slot, :, pl.ds(0, 896)], osend.at[slot])

        @pl.when(zt != z)
        def _():
            drain(stage.at[slot, :, pl.ds(0, 128)], osend.at[2 + slot])


def store_kernel(rows, out, sem):
    copy = pltpu.make_async_copy(rows, out, sem)
    copy.start()
    copy.wait()


def per_device(
    tokens, mix_gain, query_weight, key_weight, value_weight, outer_gate_weight,
    inner_gate_weight, conv_input_weight, query_gain, key_gain, gate_totals, conv_taps,
    attn_out_gain, conv_out_gain, attn_out_weight, conv_out_weight,
):
    DMA = pltpu.SemaphoreType.DMA
    far = pl.BlockSpec(memory_space=pl.ANY)
    near = pl.BlockSpec(memory_space=VMEM)
    rows = pl.pallas_call(
        layer_kernel,
        out_shape=pltpu.VMEM((128, WIDTH), BF16),
        in_specs=[far] * 16,
        out_specs=near,
        scratch_shapes=[
            VMEM((1, WIDTH), F32),
            VMEM((1, HEAD), F32),
            VMEM((1, HEAD), F32),
            VMEM((2, ROWS), F32),
            VMEM((3, 128), F32),
            VMEM((1, 128), F32),
            VMEM((1, 128), F32),
            VMEM((8, ROWS, FEATURES), BF16),
            VMEM((6, WIDTH, 128), BF16),
            VMEM((768, WIDTH), BF16),
            VMEM((4, CHUNK, WIDTH), BF16),
            VMEM((4, 1, CHUNK), F32),
            VMEM((768, CHUNK), F32),
            VMEM((128, ROWS), F32),
            VMEM((128, ROWS), BF16),
            VMEM((128, 128), BF16),
            VMEM((2, QROWS, ROWS), BF16),
            VMEM((2, KVROWS, ROWS), BF16),
            VMEM((2, HEAD, 128), F32),
            VMEM((6, 128, 128), F32),
            VMEM((2, 128, ROWS), BF16),
            VMEM((16, KVROWS, ROWS), BF16),
            VMEM((2, HEAD, 128), F32),
            VMEM((2, ROWS, 128), BF16),
            VMEM((2, ROWS, TILE), F32),
            VMEM((2, 1, ROWS), F32),
            VMEM((2, HEAD, ROWS), F32),
            VMEM((2, HEAD, ROWS), BF16),
            VMEM((128, ROWS), BF16),
            VMEM((WIDTH, WIDTH), BF16),
            VMEM((WIDTH, 128), BF16),
            VMEM((128, WIDTH), BF16),
            VMEM((128, WIDTH), F32),
            DMA((16,)), DMA((1,)), DMA((1,)), DMA((4, 4)), DMA((4,)), DMA((2,)), DMA((2, 2)),
            DMA((2,)), DMA((1,)), DMA((2,)), DMA((4,)), DMA((1,)), DMA((1,)), DMA((1,)), DMA((1,)),
            DMA((2, 4)), DMA((8, 4)), DMA((4,)), DMA((2,)), DMA((4,)), DMA((1,)), DMA((4, 2)),
            DMA((1,)), DMA((1,)), DMA((1,)),
        ],
        compiler_params=pltpu.CompilerParams(
            collective_id=1, has_side_effects=True, vmem_limit_bytes=56 * 2**20
        ),
        name="layer",
    )(
        tokens, mix_gain.reshape(1, WIDTH), query_weight, key_weight, value_weight,
        outer_gate_weight, inner_gate_weight, conv_input_weight, query_gain.reshape(1, HEAD),
        key_gain.reshape(1, HEAD), gate_totals.T, conv_taps, attn_out_gain.reshape(1, 128),
        conv_out_gain.reshape(1, 128), attn_out_weight, conv_out_weight,
    )
    return pl.pallas_call(
        store_kernel,
        out_shape=jax.ShapeDtypeStruct((128, WIDTH), BF16),
        in_specs=[near],
        out_specs=far,
        scratch_shapes=[DMA],
        name="store",
    )(pltpu.with_memory_space_constraint(rows, pltpu.VMEM))


def solution(mesh):
    placed = (
        P("sp", "tp"), P(), P(None, "tp"), P(None, "tp"), P(None, "tp"), P(None, "tp"),
        P(None, "tp"), P(None, "tp"), P(), P(), P("sp", "tp"), P(None, "tp"), P("tp"),
        P("tp"), P("tp", None), P("tp", None),
    )
    return jax.shard_map(
        per_device, mesh=mesh, in_specs=placed, out_specs=P(("sp", "tp"), None), check_vma=False
    )
```
